128 devices in a mesh: sp: 16 (over z, x), tp: 8 (over y, core).
Axes of the slice: x: 4, y: 4, z: 4, core: 2. Of those that a mesh axis runs over, the one named last changes fastest.
Arguments:
- tokens_in: bfloat16 [12288, 2048], P(('sp', 'tp')), may hold values from -300 to 300
- norm_gain: float32 [2048], replicated, may hold values from 0.1 to 1.9
- query_weight: bfloat16 [2048, 1024], P('sp', 'tp'), may hold values from -64 to 64
- key_weight: bfloat16 [2048, 512], P('sp', 'tp'), may hold values from -1 to 1
- value_weight: bfloat16 [2048, 512], P('sp', 'tp'), may hold values from -0.125 to 0.125
- pool_weight: bfloat16 [2048, 1024], P('sp', 'tp'), may hold values from -0.125 to 0.125
- sink_logit: float32 [16], P('tp'), may hold values from 1 to 5
- pool_gain: float32 [1024], P('tp'), may hold values from 0.1 to 1.9
- attention_out_weight: bfloat16 [1024, 2048], P('tp', 'sp'), may hold values from -0.125 to 0.125
- pool_out_weight: bfloat16 [1024, 2048], P('tp', 'sp'), may hold values from -0.1875 to 0.1875
Outputs:
- mixed_out: bfloat16 [12288, 2048], P(('sp', 'tp'))
The draws below stay inside these ranges and needn't reach their ends.
All inputs are finite; a program needn't handle non-finite values.
Results may differ from the reference program's by a relative error of at most 0.014.
Values may be sent and summed in bfloat16 or wider, within the bound.
A program may use at most 64 MiB of HBM per device.

```python
import jax
import jax.numpy as jnp
from jax import lax

D = 2048
HEADS = 16
KV_HEADS = 8
HEAD_DIM = 64
POOL_CH = 256
POOL_GROUPS = 4
WINDOW = 128
TOK_DEV = 768
TOKENS = 12288
Q_WIDTH = 1024
KV_WIDTH = 512
POOL_WIDTH = 1024
N_TP = 8


def draw_tokens_in(key, part):
    noise_key = jax.random.fold_in(key, 11)
    direction_key = jax.random.fold_in(key, 12)
    level_key = jax.random.fold_in(key, 13)
    rough = jax.random.normal(noise_key, (TOKENS, D), jnp.float32)
    direction = jax.random.normal(direction_key, (D,), jnp.float32)
    block_count = TOKENS // TOK_DEV
    block_number = jnp.arange(block_count)
    ramp = block_number.astype(jnp.float32) / max(block_count - 1, 1)
    alternate = (1 - 2 * (block_number % 2)).astype(jnp.float32)
    jitter = jax.random.uniform(level_key, (block_count,), jnp.float32, 0.8, 1.3)
    levels = 2.0 * 3.0 ** ramp * jitter * alternate
    level_rows = jnp.repeat(levels, TOK_DEV)
    values = rough + level_rows[:, None] * direction[None, :]
    return jnp.clip(values, -300.0, 300.0).astype(jnp.bfloat16)


def key_base(key):
    limit = 6.0 * D ** (-0.5)
    base = jax.random.normal(jax.random.fold_in(key, 71), (D, KV_HEADS * HEAD_DIM), jnp.float32) * D ** (-0.5)
    base = jnp.clip(base, -limit, limit)
    return base


def draw_key_weight(key, part):
    return jnp.clip(key_base(key), -1.0, 1.0).astype(jnp.bfloat16)


def draw_query_weight(key, part):
    limit = 6.0 * D ** (-0.5)
    own = jax.random.normal(jax.random.fold_in(key, 72), (D, HEADS * HEAD_DIM), jnp.float32) * D ** (-0.5)
    own = jnp.clip(own, -limit, limit)
    return jnp.clip(own, -64.0, 64.0).astype(jnp.bfloat16)


def with_spikes(values, key, source, target, blocks, factor):
    owner, partner = [(jnp.arange(values.shape[dim]) // (values.shape[dim] // blocks)).reshape([-1 if axis == dim else 1 for axis in range(values.ndim)]) for dim in (source, target)]
    chosen = jax.random.permutation(key, blocks)[partner]
    strong = (owner == chosen) | (owner == (partner + blocks // 2) % blocks)
    return jnp.where(strong, factor * values, values)


def level_of(key, shape, split, low, largest):
    level = 1.0
    for dim, shards_of in split:
        steps = jax.random.uniform(jax.random.fold_in(jax.random.fold_in(key, 6), dim), (shards_of,), jnp.float32, low / len(split), largest / len(split))
        level = level * jnp.repeat(jnp.exp(steps), shape[dim] // shards_of).reshape((-1,) + (1,) * (len(shape) - 1 - dim))
    return level


def bell_draw(stream_key, dims, deviation, most, pieces=(), held_as=jnp.bfloat16):
    drawn = deviation * jax.random.normal(stream_key, dims, jnp.float32)
    if pieces:
        drawn = drawn * level_of(stream_key, dims, pieces, -0.22, 0.18)
    return jnp.clip(drawn, -most, most).astype(held_as)


def bell_draw_with(rng, dims, deviation, bound, shards, heavy, dtype=jnp.bfloat16):
    drawn = deviation * jax.random.normal(rng, dims, jnp.float32)
    if shards:
        drawn = drawn * level_of(rng, dims, shards, -0.22, 0.18)
    return jnp.clip(with_spikes(drawn, jax.random.fold_in(rng, 3), *heavy), -bound, bound).astype(dtype)


def setup_inputs(seed: int = 0) -> dict:
    keys = jax.random.split(jax.random.key(seed), 11)
    return {
        "tokens_in": draw_tokens_in(jax.random.fold_in(keys[10], 71), 0),
        "norm_gain": jnp.clip(1.0 + 0.18 * jax.random.normal(keys[1], (D,), jnp.float32), 0.1, 1.9),
        "query_weight": draw_query_weight(jax.random.fold_in(keys[10], 71), 0),
        "key_weight": draw_key_weight(jax.random.fold_in(keys[10], 71), 0),
        "value_weight": bell_draw(keys[4], (D, KV_WIDTH), D ** -0.5, 0.125, ((0, 16), (1, 8))),
        "pool_weight": bell_draw(keys[5], (D, POOL_WIDTH), D ** -0.5, 0.125, ((0, 16), (1, 8))),
        "sink_logit": jnp.clip(1.0 + 4.0 * jax.random.uniform(keys[6], (HEADS,), jnp.float32) ** level_of(keys[6], (HEADS,), ((0, 8),), -0.2, 0.2), 1.0, 5.0),
        "pool_gain": jnp.clip(1.0 + 0.18 * jax.random.normal(keys[7], (POOL_WIDTH,), jnp.float32), 0.1, 1.9),
        "attention_out_weight": bell_draw(keys[8], (Q_WIDTH, D), (Q_WIDTH + POOL_WIDTH) ** -0.5, 0.125, ((0, 8), (1, 16))),
        "pool_out_weight": bell_draw_with(keys[9], (POOL_WIDTH, D), (Q_WIDTH + POOL_WIDTH) ** -0.5, 0.1875, ((0, 8), (1, 16)), (0, 1, 16, 2.0)),
    }


EPS = 1e-06
SHORT_REACHES = (8, 32)

def attention_mix(query_rows, key_rows, value_rows, sink_logit):
    total_rows = query_rows.shape[0]
    blocks = total_rows // WINDOW
    group = HEADS // KV_HEADS
    queries = query_rows.astype(jnp.float32).reshape(blocks, WINDOW, KV_HEADS, group, HEAD_DIM)
    key_blocks = key_rows.astype(jnp.float32).reshape(blocks, WINDOW, KV_HEADS, HEAD_DIM)
    value_blocks = value_rows.astype(jnp.float32).reshape(blocks, WINDOW, KV_HEADS, HEAD_DIM)

    def with_previous(blocks_in):
        earlier = jnp.concatenate([jnp.zeros_like(blocks_in[:1]), blocks_in[:-1]], axis=0)
        return jnp.concatenate([earlier, blocks_in], axis=1)
    key_pairs = with_previous(key_blocks)
    value_pairs = with_previous(value_blocks)
    scores = jnp.einsum('nqhgd,nkhd->nhgqk', queries, key_pairs) * HEAD_DIM ** (-0.5)
    q_index = jnp.arange(WINDOW)[:, None]
    k_index = jnp.arange(2 * WINDOW)[None, :]
    distance = q_index + WINDOW - k_index
    inside = (distance >= 0) & (distance < WINDOW)
    block_index = jnp.arange(blocks)[:, None, None]
    allowed = inside[None] & ((block_index > 0) | (k_index >= WINDOW)[None])
    scores = jnp.where(allowed[:, None, None], scores, -jnp.inf)
    sinks = sink_logit.astype(jnp.float32).reshape(1, KV_HEADS, group, 1, 1)
    peak = jnp.maximum(lax.optimization_barrier(jnp.max(scores, axis=-1, keepdims=True)), sinks)
    expo = jnp.exp(scores - peak)
    denom = lax.optimization_barrier(jnp.sum(expo, axis=-1, keepdims=True)) + jnp.exp(sinks - peak)
    probs = lax.optimization_barrier((expo / denom).astype(jnp.bfloat16))
    attended = jnp.einsum('nhgqk,nkhd->nqhgd', probs.astype(jnp.float32), value_pairs)
    return attended.astype(jnp.bfloat16).reshape(total_rows, HEADS * HEAD_DIM)

def pool_mix(pool_rows, pool_gain):
    total_rows = pool_rows.shape[0]
    values = pool_rows.astype(jnp.float32)
    running = jnp.concatenate([jnp.zeros((1, values.shape[1]), jnp.float32), jnp.cumsum(values, axis=0)], axis=0)
    position = jnp.arange(total_rows)
    outputs = []
    for group_index, reach in enumerate(SHORT_REACHES + (WINDOW,)):
        span = running[:, group_index * POOL_CH:(group_index + 1) * POOL_CH]
        lower = span[jnp.maximum(position + 1 - reach, 0)]
        count = jnp.minimum(position + 1, reach).astype(jnp.float32)[:, None]
        outputs.append((span[1:] - lower) / count)
    whole_prefix = running[1:, (POOL_GROUPS - 1) * POOL_CH:] / (position + 1).astype(jnp.float32)[:, None]
    pooled = jnp.concatenate(outputs + [whole_prefix], axis=1)
    return ((pooled - values) * pool_gain.astype(jnp.float32)).astype(jnp.bfloat16)

def reference(tokens_in, norm_gain, query_weight, key_weight, value_weight, pool_weight, sink_logit, pool_gain, attention_out_weight, pool_out_weight):
    widened = tokens_in.astype(jnp.float32)
    inverse = lax.rsqrt(lax.optimization_barrier(jnp.mean(widened * widened, axis=1, keepdims=True)) + EPS)
    normed = (widened * inverse * norm_gain.astype(jnp.float32)).astype(jnp.bfloat16)
    query_rows = jnp.dot(normed, query_weight, preferred_element_type=jnp.float32).astype(jnp.bfloat16)
    key_rows = jnp.dot(normed, key_weight, preferred_element_type=jnp.float32).astype(jnp.bfloat16)
    value_rows = jnp.dot(normed, value_weight, preferred_element_type=jnp.float32).astype(jnp.bfloat16)
    pool_rows = jnp.dot(normed, pool_weight, preferred_element_type=jnp.float32).astype(jnp.bfloat16)
    attended = attention_mix(query_rows, key_rows, value_rows, sink_logit)
    pool_mixed = pool_mix(pool_rows, pool_gain)
    attend_cols = Q_WIDTH // N_TP
    pool_cols = POOL_WIDTH // N_TP
    summed = jnp.zeros((tokens_in.shape[0], D), jnp.float32)
    for block in range(N_TP):
        partial_sum = jnp.dot(attended[:, block * attend_cols:(block + 1) * attend_cols], attention_out_weight[block * attend_cols:(block + 1) * attend_cols], preferred_element_type=jnp.float32)
        partial_sum = partial_sum + jnp.dot(pool_mixed[:, block * pool_cols:(block + 1) * pool_cols], pool_out_weight[block * pool_cols:(block + 1) * pool_cols], preferred_element_type=jnp.float32)
        rounded = lax.optimization_barrier(partial_sum.astype(jnp.bfloat16))
        summed = summed + rounded.astype(jnp.float32)
    return summed.astype(jnp.bfloat16)
```

```python
import jax
import jax.numpy as jnp
from jax import lax
from jax.experimental import pallas as pl
from jax.experimental.pallas import tpu as pltpu
from jax.sharding import PartitionSpec as P

MESH = pl.DeviceIdType.MESH
F32 = jnp.float32
BF16 = jnp.bfloat16

D = 2048
HEAD_DIM = 64
WINDOW = 128
EPS = 1e-06
SIDE = 4
PLANE = SIDE * SIDE
BLOCK = 96
HALF = BLOCK // 2
ROWS = 2 * SIDE * BLOCK
CHUNK = 2 * BLOCK
DEPTH = D // PLANE
IN_COLS = 384
N_MSG = 144


class Messages:
    def __init__(self, send_sems, recv_sems):
        self.send_sems, self.recv_sems, self.made = send_sems, recv_sems, []

    def new(self, src, dst, device, land):
        number = len(self.made)
        message = Message(
            lambda a, b: pltpu.make_async_remote_copy(
                src_ref=a,
                dst_ref=b,
                send_sem=self.send_sems.at[number],
                recv_sem=self.recv_sems.at[number],
                device_id=device,
                device_id_type=MESH,
            ),
            src,
            dst,
            land,
        )
        self.made.append(message)
        return message


class Message:
    def __init__(self, make, src, dst, land):
        self.make, self.src, self.dst, self.land = make, src, dst, land

    def start(self):
        self.make(self.src, self.dst).start()

    def arrived(self):
        self.make(self.land, self.land).wait_recv()

    def sent(self):
        self.make(self.src, self.dst).wait_send()


def rows_of(start, size, unit=16):
    return pl.ds(pl.multiple_of(start, unit), size)


def kernel(
    x_hbm,
    gain_hbm,
    wq_hbm,
    wk_hbm,
    wv_hbm,
    wp_hbm,
    sink_ref,
    pgain_hbm,
    wa_hbm,
    wo_hbm,
    out_ref,
    xin,
    gain,
    pgain,
    wk,
    wv,
    tok,
    win,
    wout,
    qbuf,
    kvsend,
    kvland,
    kp0,
    kp1,
    vp0,
    vp1,
    pext,
    tot,
    tots,
    sraw,
    amine,
    apart,
    far,
    nbn,
    nbp,
    accn,
    accp,
    rfn,
    rfp,
    rn,
    rp,
    local_sems,
    send_sems,
    recv_sems,
):
    sp = lax.axis_index("sp")
    tp = lax.axis_index("tp")
    z, x = sp // SIDE, lax.rem(sp, SIDE)
    y, c = tp // 2, lax.rem(tp, 2)
    other = 1 - c

    def turn(i, by):
        return lax.rem(i + by + SIDE, SIDE)

    yn, yp, yf = turn(y, 1), turn(y, -1), turn(y, 2)
    partner = (sp, y * 2 + other)
    up, down = (sp, yn * 2 + c), (sp, yp * 2 + c)

    own_in = rows_of(sp * DEPTH, DEPTH, 128)
    own_cols = rows_of(sp * 128, 128, 128)
    loads = [
        (x_hbm, xin),
        (gain_hbm, gain),
        (wk_hbm, wk),
        (wv_hbm, wv),
        (wq_hbm, win.at[own_in, pl.ds(0, 128)]),
        (wp_hbm, win.at[own_in, pl.ds(256, 128)]),
        (pgain_hbm, pgain),
        (wa_hbm, wout.at[pl.ds(0, 128), own_cols]),
        (wo_hbm, wout.at[pl.ds(128, 128), own_cols]),
    ]
    loads = [pltpu.make_async_copy(a, b, local_sems.at[n]) for n, (a, b) in enumerate(loads)]
    for load in loads:
        load.start()

    barrier = pltpu.get_barrier_semaphore()
    for step in range(1, PLANE):
        peer = (lax.rem(sp + step, PLANE), tp)
        pl.semaphore_signal(barrier, inc=1, device_id=peer, device_id_type=MESH)
    for peer in (up, down, partner):
        pl.semaphore_signal(barrier, inc=1, device_id=peer, device_id_type=MESH)

    loads[0].wait()
    loads[1].wait()
    gains = gain[...]
    for r in range(0, BLOCK, 16):
        wide = xin[pl.ds(r, 16)].astype(F32)
        inverse = lax.rsqrt(jnp.mean(wide * wide, axis=1, keepdims=True) + EPS)
        tok[rows_of(tp * BLOCK + r, 16), :] = (wide * inverse * gains).astype(BF16)
    loads[2].wait()
    loads[3].wait()
    win[own_in, pl.ds(128, 128)] = jnp.concatenate([wk[...], wv[...]], axis=1)
    for load in loads[4:]:
        load.wait()

    messages = Messages(send_sems, recv_sems)

    def block(yy, cc):
        return tok.at[rows_of((yy * 2 + cc) * BLOCK, BLOCK)]

    def half(yy, cc, h):
        return tok.at[rows_of((yy * 2 + cc) * BLOCK + h * HALF, HALF)]

    t_n0 = messages.new(half(y, c, 0), half(y, c, 0), up, half(yp, c, 0))
    t_p1 = messages.new(half(y, c, 1), half(y, c, 1), down, half(yn, c, 1))
    t_n1 = messages.new(half(y, c, 1), half(y, c, 1), up, half(yp, c, 1))
    t_p0 = messages.new(half(y, c, 0), half(y, c, 0), down, half(yn, c, 0))
    f_n = messages.new(half(yp, c, 0), half(yp, c, 0), up, half(yf, c, 0))
    f_p = messages.new(half(yn, c, 1), half(yn, c, 1), down, half(yf, c, 1))
    d_own = messages.new(block(y, c), block(y, c), partner, block(y, other))

    def across(yy, h):
        return messages.new(half(yy, c, h), half(yy, c, h), partner, half(yy, other, h))

    d_p0, d_n1, d_p1, d_n0 = across(yp, 0), across(yn, 1), across(yp, 1), across(yn, 0)
    d_f0, d_f1 = across(yf, 0), across(yf, 1)

    class Gather:
        def __init__(self, group, piece, sub):
            def source(o1, o2):
                if group == 0:
                    return turn(z, o2) * SIDE + turn(x, o1)
                return turn(z, o1) * SIDE + turn(x, o2)

            def device(o1, o2):
                return (source(o1, o2), tp)

            def send(ref, o1, o2, land):
                return messages.new(ref, ref, device(o1, o2), land)

            s = source
            self.a_n = send(piece(s(0, 0)), 1, 0, piece(s(-1, 0)))
            self.a_p = send(piece(s(0, 0)), -1, 0, piece(s(1, 0)))
            self.a_fn = send(sub(s(-1, 0), 0), 1, 0, sub(s(2, 0), 0))
            self.a_fp = send(sub(s(1, 0), 1), -1, 0, sub(s(2, 0), 1))
            self.b_n, self.b_p, self.b_fn, self.b_fp = {}, {}, {}, {}
            for o in (0, -1, 1, 2):
                self.b_n[o] = send(piece(s(o, 0)), 0, 1, piece(s(o, -1)))
                self.b_p[o] = send(piece(s(o, 0)), 0, -1, piece(s(o, 1)))
                self.b_fn[o] = send(sub(s(o, -1), 0), 0, 1, sub(s(o, 2), 0))
                self.b_fp[o] = send(sub(s(o, 1), 1), 0, -1, sub(s(o, 2), 1))

        def begin(self):
            self.a_n.start()
            self.a_p.start()
            self.cross(0)

        def cross(self, o):
            self.b_n[o].start()
            self.b_p[o].start()

        def near(self):
            self.a_n.arrived()
            self.a_fn.start()
            self.a_p.arrived()
            self.a_fp.start()
            self.cross(-1)
            self.cross(1)

        def distant(self):
            self.a_fn.arrived()
            self.a_fp.arrived()
            self.cross(2)

        def pass_on(self, o):
            self.b_n[o].arrived()
            self.b_fn[o].start()
            self.b_p[o].arrived()
            self.b_fp[o].start()

        def finish(self):
            for o in (0, -1, 1, 2):
                self.b_fn[o].arrived()
                self.b_fp[o].arrived()

    def in_piece(group):
        size = DEPTH // 2
        return (
            lambda s: win.at[rows_of(s * DEPTH + group * size, size)],
            lambda s, h: win.at[rows_of(s * DEPTH + group * size + h * (size // 2), size // 2)],
        )

    def out_piece(group):
        return (
            lambda s: wout.at[pl.ds(group * 128, 128), rows_of(s * 128, 128, 128)],
            lambda s, h: wout.at[pl.ds(group * 128 + h * 64, 64), rows_of(s * 128, 128, 128)],
        )

    ins = [Gather(g, *in_piece(g)) for g in range(2)]
    outs = [Gather(g, *out_piece(g)) for g in range(2)]
    d_out = messages.new(
        wout.at[pl.ds(0, 256)], wout.at[pl.ds(256, 256)], partner, wout.at[pl.ds(256, 256)]
    )

    pl.semaphore_wait(barrier, PLANE - 1 + 3)

    for m in (t_n0, t_p1, t_n1, t_p0):
        m.start()
    for g in ins:
        g.begin()
    d_own.start()
    for g in ins:
        g.near()
    for g in ins:
        g.pass_on(0)
    for g in ins:
        g.distant()
    t_n0.arrived()
    f_n.start()
    d_p0.start()
    t_p1.arrived()
    f_p.start()
    d_n1.start()
    for g in ins:
        g.pass_on(-1)
        g.pass_on(1)
    for g in ins:
        g.pass_on(2)
    for g in outs:
        g.begin()
    for g in outs:
        g.near()
    for g in outs:
        g.pass_on(0)
    for g in outs:
        g.distant()
    for g in ins:
        g.finish()
    t_n1.arrived()
    d_p1.start()
    t_p0.arrived()
    d_n0.start()

    lane = lax.broadcasted_iota(jnp.int32, (CHUNK, 128), 1)

    def spread(kv, rows, at):
        first = lax.broadcasted_iota(jnp.int32, (rows, 128), 1) < HEAD_DIM
        turned = pltpu.roll(kv, HEAD_DIM, 1)
        kp0[at, :] = jnp.where(first, kv, 0.0).astype(BF16)
        kp1[at, :] = jnp.where(first, 0.0, turned).astype(BF16)
        vp0[at, :] = jnp.where(first, turned, 0.0).astype(BF16)
        vp1[at, :] = jnp.where(first, 0.0, kv).astype(BF16)

    def project(yy):
        at = rows_of(yy * CHUNK, CHUNK)
        got = jnp.dot(tok[at, :], win[...], preferred_element_type=F32)
        qbuf[at, :] = got[:, :128].astype(BF16)
        ahead = rows_of(yy * CHUNK + WINDOW, CHUNK)
        spread(got[:, 128:256].astype(BF16).astype(F32), CHUNK, ahead)
        pool = got[:, 256:].astype(BF16)
        pext[ahead, :] = pool
        return jnp.sum(pool.astype(F32).reshape(CHUNK // 8, 8, 128), axis=0)

    d_own.arrived()
    total = project(y)
    for g in outs:
        g.pass_on(-1)
        g.pass_on(1)
    d_p0.arrived()
    d_p1.arrived()
    total = total + project(yp)
    for g in outs:
        g.pass_on(2)
    d_n0.arrived()
    d_n1.arrived()
    total = total + project(yn)
    for g in outs:
        g.finish()
    d_out.start()
    f_n.arrived()
    d_f0.start()
    f_p.arrived()
    d_f1.start()
    d_f0.arrived()
    d_f1.arrived()
    total = total + project(yf)

    last = pl.ds(ROWS, WINDOW)
    kvsend[...] = kp0[last, :] + vp1[last, :]
    after = (lax.rem(sp + 1, PLANE), tp)
    h_kv = messages.new(kvsend, kvland, after, kvland)
    h_p = messages.new(pext.at[last], pext.at[pl.ds(0, WINDOW)], after, pext.at[pl.ds(0, WINDOW)])
    h_kv.start()
    h_p.start()
    tot[...] = total
    sums = []
    for step in range(1, PLANE):
        m = messages.new(
            tot,
            tots.at[sp],
            (lax.rem(sp + step, PLANE), tp),
            tots.at[lax.rem(sp + PLANE - step, PLANE)],
        )
        m.start()
        sums.append(m)
    tots[sp] = total

    q_index = lax.broadcasted_iota(jnp.int32, (WINDOW, 2 * WINDOW), 0)
    k_index = lax.broadcasted_iota(jnp.int32, (WINDOW, 2 * WINDOW), 1)
    distance = q_index + WINDOW - k_index
    reach = jnp.where(y == 0, 8, jnp.where(y == 1, 32, jnp.where(y == 2, WINDOW, 1 << 24)))
    inside = (distance >= 0) & (distance < WINDOW)
    banded = (distance >= 0) & (distance < reach) & ((k_index >= WINDOW) | (y < 3))
    sinks = (sink_ref[0], sink_ref[1])

    def probabilities(q, keys, allowed, sink):
        scores = lax.dot_general(q, keys, (((1,), (1,)), ((), ())), preferred_element_type=F32)
        scores = jnp.where(allowed, scores * HEAD_DIM ** (-0.5), -jnp.inf)
        peak = jnp.maximum(jnp.max(scores, axis=1, keepdims=True), sink)
        expo = jnp.exp(scores - peak)
        denom = jnp.sum(expo, axis=1, keepdims=True) + jnp.exp(sink - peak)
        return (expo * (1.0 / denom)).astype(BF16)

    def attend(b):
        at, pair = pl.ds(b * WINDOW, WINDOW), pl.ds(b * WINDOW, 2 * WINDOW)
        allowed, band = inside, banded
        if b == 0:
            present = (k_index >= WINDOW) | (sp > 0)
            allowed, band = allowed & present, band & present
        q = qbuf[at, :]
        p0 = probabilities(q, kp0[pair, :], allowed, sinks[0])
        p1 = probabilities(q, kp1[pair, :], allowed, sinks[1])
        mixed = jnp.dot(p0, vp0[pair, :], preferred_element_type=F32)
        mixed = mixed + jnp.dot(p1, vp1[pair, :], preferred_element_type=F32)
        amine[at, pl.ds(0, 128)] = mixed.astype(BF16)
        ones = jnp.where(band, 1.0, 0.0).astype(BF16)
        sraw[at, :] = jnp.dot(ones, pext[pair, :], preferred_element_type=F32)

    for b in range(1, ROWS // WINDOW):
        attend(b)
    h_kv.arrived()
    h_p.arrived()
    spread(kvland[...].astype(F32), WINDOW, pl.ds(0, WINDOW))
    attend(0)

    for m in sums:
        m.arrived()
    earlier = lax.broadcasted_iota(jnp.int32, (PLANE, 8, 128), 0) < sp
    before = jnp.sum(jnp.sum(jnp.where(earlier, tots[...], 0.0), axis=0), axis=0, keepdims=True)
    carry = jnp.where(y == 3, before, 0.0)
    pool_gain = pgain[...]
    for b in range(ROWS // WINDOW):
        at = pl.ds(b * WINDOW, WINDOW)
        position = sp * ROWS + b * WINDOW + lax.broadcasted_iota(jnp.int32, (WINDOW, 128), 0)
        count = jnp.minimum(position + 1, reach).astype(F32)
        here = sraw[at, :]
        value = pext[pl.ds((b + 1) * WINDOW, WINDOW), :].astype(F32)
        amine[at, pl.ds(128, 128)] = (((here + carry) / count - value) * pool_gain).astype(BF16)
        carry = carry + jnp.where(y == 3, here[WINDOW - 1 :, :], 0.0)

    swaps = []
    for yy in (yf, yn, yp, y):
        src = amine.at[rows_of((yy * 2 + other) * BLOCK, BLOCK)]
        dst = apart.at[rows_of(yy * BLOCK, BLOCK)]
        m = messages.new(src, dst, partner, dst)
        m.start()
        swaps.append(m)
    d_out.arrived()

    def product(yy, put):
        mine = amine[rows_of((yy * 2 + c) * BLOCK, BLOCK), :]
        theirs = apart[rows_of(yy * BLOCK, BLOCK), :]
        for n in range(0, D, 512):
            cols = pl.ds(n, 512)
            got = jnp.dot(mine, wout[pl.ds(0, 256), cols], preferred_element_type=F32)
            got = got + jnp.dot(theirs, wout[pl.ds(256, 256), cols], preferred_element_type=F32)
            put(cols, got)

    top, bottom = pl.ds(0, HALF), pl.ds(HALF, HALF)
    r_fn = messages.new(far.at[top], rfn, up, rfn)
    r_fp = messages.new(far.at[bottom], rfp, down, rfp)
    r_n1 = messages.new(nbn.at[bottom], rn.at[bottom], up, rn.at[bottom])
    r_p0 = messages.new(nbp.at[top], rp.at[top], down, rp.at[top])
    r_n0 = messages.new(nbn.at[top], rn.at[top], up, rn.at[top])
    r_p1 = messages.new(nbp.at[bottom], rp.at[bottom], down, rp.at[bottom])

    def put_far(cols, got):
        far[:, cols] = got.astype(BF16)

    def put_next(cols, got):
        nbn[bottom, cols] = got[HALF:].astype(BF16)
        accn[:, cols] = got[:HALF]

    def put_prev(cols, got):
        nbp[top, cols] = got[:HALF].astype(BF16)
        accp[:, cols] = got[HALF:]

    swaps[0].arrived()
    product(yf, put_far)
    r_fn.start()
    r_fp.start()
    swaps[1].arrived()
    product(yn, put_next)
    r_n1.start()
    swaps[2].arrived()
    product(yp, put_prev)
    r_p0.start()
    r_fn.arrived()
    nbn[top, :] = (accn[...] + rfn[...].astype(F32)).astype(BF16)
    r_n0.start()
    r_fp.arrived()
    nbp[bottom, :] = (accp[...] + rfp[...].astype(F32)).astype(BF16)
    r_p1.start()

    swaps[3].arrived()

    def put_own(cols, got):
        accn[:, cols] = got[:HALF]
        accp[:, cols] = got[HALF:]

    product(y, put_own)
    r_n1.arrived()
    accp[...] = accp[...] + rn[bottom, :].astype(F32)
    r_p0.arrived()
    accn[...] = accn[...] + rp[top, :].astype(F32)
    r_n0.arrived()
    out_ref[top, :] = (accn[...] + rn[top, :].astype(F32)).astype(BF16)
    r_p1.arrived()
    out_ref[bottom, :] = (accp[...] + rp[bottom, :].astype(F32)).astype(BF16)
    for m in messages.made:
        m.sent()
    assert len(messages.made) <= N_MSG


def local(
    tokens_in,
    norm_gain,
    query_weight,
    key_weight,
    value_weight,
    pool_weight,
    sink_logit,
    pool_gain,
    attention_out_weight,
    pool_out_weight,
):
    hbm = pl.BlockSpec(memory_space=pl.ANY)
    scratch = [
        ((BLOCK, D), BF16),
        ((1, D), F32),
        ((1, 128), F32),
        ((DEPTH, 64), BF16),
        ((DEPTH, 64), BF16),
        ((ROWS, D), BF16),
        ((D, IN_COLS), BF16),
        ((512, D), BF16),
        ((ROWS, 128), BF16),
        ((WINDOW, 128), BF16),
        ((WINDOW, 128), BF16),
        ((ROWS + WINDOW, 128), BF16),
        ((ROWS + WINDOW, 128), BF16),
        ((ROWS + WINDOW, 128), BF16),
        ((ROWS + WINDOW, 128), BF16),
        ((ROWS + WINDOW, 128), BF16),
        ((8, 128), F32),
        ((PLANE, 8, 128), F32),
        ((ROWS, 128), F32),
        ((ROWS, 256), BF16),
        ((SIDE * BLOCK, 256), BF16),
        ((BLOCK, D), BF16),
        ((BLOCK, D), BF16),
        ((BLOCK, D), BF16),
        ((HALF, D), F32),
        ((HALF, D), F32),
        ((HALF, D), BF16),
        ((HALF, D), BF16),
        ((BLOCK, D), BF16),
        ((BLOCK, D), BF16),
    ]
    return pl.pallas_call(
        kernel,
        out_shape=jax.ShapeDtypeStruct((BLOCK, D), BF16),
        in_specs=[hbm] * 6 + [pl.BlockSpec(memory_space=pltpu.SMEM)] + [hbm] * 3,
        out_specs=pl.BlockSpec(memory_space=pltpu.VMEM),
        scratch_shapes=[pltpu.VMEM(shape, kind) for shape, kind in scratch]
        + [
            pltpu.SemaphoreType.DMA((9,)),
            pltpu.SemaphoreType.DMA((N_MSG,)),
            pltpu.SemaphoreType.DMA((N_MSG,)),
        ],
        compiler_params=pltpu.CompilerParams(
            collective_id=0, has_side_effects=True, vmem_limit_bytes=40 * 1024 * 1024
        ),
    )(
        tokens_in,
        norm_gain.reshape(1, D),
        query_weight,
        key_weight,
        value_weight,
        pool_weight,
        sink_logit,
        pool_gain.reshape(1, 128),
        attention_out_weight,
        pool_out_weight,
    )


def solution(mesh):
    in_specs = (
        P(("sp", "tp"), None),
        P(),
        P("sp", "tp"),
        P("sp", "tp"),
        P("sp", "tp"),
        P("sp", "tp"),
        P("tp"),
        P("tp"),
        P("tp", "sp"),
        P("tp", "sp"),
    )
    out_specs = P(("sp", "tp"), None)
    return jax.shard_map(local, mesh=mesh, in_specs=in_specs, out_specs=out_specs, check_vma=False)
```

```python
import jax
import jax.numpy as jnp
from jax import lax
from jax.experimental import pallas as pl
from jax.experimental.pallas import tpu as pltpu
from jax.sharding import PartitionSpec as P

MESH = pl.DeviceIdType.MESH
F32 = jnp.float32
BF16 = jnp.bfloat16

D = 2048
HEAD_DIM = 64
WINDOW = 128
EPS = 1e-06
SIDE = 4
PLANE = SIDE * SIDE
BLOCK = 96
HALF = BLOCK // 2
ROWS = 2 * SIDE * BLOCK
CHUNK = 2 * BLOCK
DEPTH = D // PLANE
IN_COLS = 384
N_MSG = 144


class Messages:
    def __init__(self, send_sems, recv_sems):
        self.send_sems, self.recv_sems, self.made = send_sems, recv_sems, []

    def new(self, src, dst, device, land):
        number = len(self.made)
        message = Message(
            lambda a, b: pltpu.make_async_remote_copy(
                src_ref=a,
                dst_ref=b,
                send_sem=self.send_sems.at[number],
                recv_sem=self.recv_sems.at[number],
                device_id=device,
                device_id_type=MESH,
            ),
            src,
            dst,
            land,
        )
        self.made.append(message)
        return message


class Message:
    def __init__(self, make, src, dst, land):
        self.make, self.src, self.dst, self.land = make, src, dst, land

    def start(self):
        self.make(self.src, self.dst).start()

    def arrived(self):
        self.make(self.land, self.land).wait_recv()

    def sent(self):
        self.make(self.src, self.dst).wait_send()


def rows_of(start, size, unit=16):
    return pl.ds(pl.multiple_of(start, unit), size)


def kernel(
    x_hbm,
    gain_hbm,
    wq_hbm,
    wk_hbm,
    wv_hbm,
    wp_hbm,
    sink_ref,
    pgain_hbm,
    wa_hbm,
    wo_hbm,
    out_ref,
    xin,
    gain,
    pgain,
    wkv,
    tok,
    win,
    wout,
    qbuf,
    kvsend,
    kvland,
    kp0,
    kp1,
    vp0,
    vp1,
    pext,
    tot,
    tots,
    sraw,
    amine,
    apart,
    far,
    nbn,
    nbp,
    accn,
    accp,
    rfn,
    rfp,
    rn,
    rp,
    local_sems,
    send_sems,
    recv_sems,
):
    sp = lax.axis_index("sp")
    tp = lax.axis_index("tp")
    z, x = sp // SIDE, lax.rem(sp, SIDE)
    y, c = tp // 2, lax.rem(tp, 2)
    other = 1 - c

    def turn(i, by):
        return lax.rem(i + by + SIDE, SIDE)

    yn, yp, yf = turn(y, 1), turn(y, -1), turn(y, 2)
    partner = (sp, y * 2 + other)
    up, down = (sp, yn * 2 + c), (sp, yp * 2 + c)

    barrier = pltpu.get_barrier_semaphore()
    beside = [(z * SIDE + turn(x, by), tp) for by in (1, -1)]
    above = [(turn(z, by) * SIDE + x, tp) for by in (1, -1)]
    peers = [up, down, partner] + beside + above
    for peer in peers:
        pl.semaphore_signal(barrier, inc=1, device_id=peer, device_id_type=MESH)

    own_in = rows_of(sp * DEPTH, DEPTH, 128)
    own_cols = rows_of(sp * 128, 128, 128)
    loads = [
        (x_hbm, xin),
        (gain_hbm, gain),
        (wk_hbm, wkv.at[pl.ds(0, HEAD_DIM)]),
        (wv_hbm, wkv.at[pl.ds(HEAD_DIM, HEAD_DIM)]),
        (wq_hbm, win.at[own_in, pl.ds(0, 128)]),
        (wp_hbm, win.at[own_in, pl.ds(256, 128)]),
        (pgain_hbm, pgain),
        (wa_hbm, wout.at[pl.ds(0, 128), own_cols]),
        (wo_hbm, wout.at[pl.ds(128, 128), own_cols]),
    ]
    loads = [pltpu.make_async_copy(a, b, local_sems.at[n]) for n, (a, b) in enumerate(loads)]
    for load in loads:
        load.start()

    loads[0].wait()
    loads[1].wait()
    gains = gain[...]
    for r in range(0, BLOCK, 16):
        wide = xin[pl.ds(r, 16)].astype(F32)
        inverse = lax.rsqrt(jnp.mean(wide * wide, axis=1, keepdims=True) + EPS)
        tok[rows_of(tp * BLOCK + r, 16), :] = (wide * inverse * gains).astype(BF16)
    loads[2].wait()
    loads[3].wait()
    win[own_in, pl.ds(128, 128)] = wkv[...].T
    for load in loads[4:]:
        load.wait()

    messages = Messages(send_sems, recv_sems)


    def block(yy, cc):
        return tok.at[rows_of((yy * 2 + cc) * BLOCK, BLOCK)]

    def half(yy, cc, h):
        return tok.at[rows_of((yy * 2 + cc) * BLOCK + h * HALF, HALF)]

    t_n0 = messages.new(half(y, c, 0), half(y, c, 0), up, half(yp, c, 0))
    t_p1 = messages.new(half(y, c, 1), half(y, c, 1), down, half(yn, c, 1))
    t_n1 = messages.new(half(y, c, 1), half(y, c, 1), up, half(yp, c, 1))
    t_p0 = messages.new(half(y, c, 0), half(y, c, 0), down, half(yn, c, 0))
    f_n = messages.new(half(yp, c, 0), half(yp, c, 0), up, half(yf, c, 0))
    f_p = messages.new(half(yn, c, 1), half(yn, c, 1), down, half(yf, c, 1))
    d_own = messages.new(block(y, c), block(y, c), partner, block(y, other))

    def across(yy, h):
        return messages.new(half(yy, c, h), half(yy, c, h), partner, half(yy, other, h))

    d_p0, d_n1, d_p1, d_n0 = across(yp, 0), across(yn, 1), across(yp, 1), across(yn, 0)
    d_f0, d_f1 = across(yf, 0), across(yf, 1)

    class Gather:
        def __init__(self, group, piece, sub):
            def source(o1, o2):
                if group == 0:
                    return turn(z, o2) * SIDE + turn(x, o1)
                return turn(z, o1) * SIDE + turn(x, o2)

            def device(o1, o2):
                return (source(o1, o2), tp)

            def send(ref, o1, o2, land):
                return messages.new(ref, ref, device(o1, o2), land)

            s = source
            self.a_n = send(piece(s(0, 0)), 1, 0, piece(s(-1, 0)))
            self.a_p = send(piece(s(0, 0)), -1, 0, piece(s(1, 0)))
            self.a_fn = send(sub(s(-1, 0), 0), 1, 0, sub(s(2, 0), 0))
            self.a_fp = send(sub(s(1, 0), 1), -1, 0, sub(s(2, 0), 1))
            self.b_n, self.b_p, self.b_fn, self.b_fp = {}, {}, {}, {}
            for o in (0, -1, 1, 2):
                self.b_n[o] = send(piece(s(o, 0)), 0, 1, piece(s(o, -1)))
                self.b_p[o] = send(piece(s(o, 0)), 0, -1, piece(s(o, 1)))
                self.b_fn[o] = send(sub(s(o, -1), 0), 0, 1, sub(s(o, 2), 0))
                self.b_fp[o] = send(sub(s(o, 1), 1), 0, -1, sub(s(o, 2), 1))

        def begin(self):
            self.a_n.start()
            self.a_p.start()
            self.cross(0)

        def cross(self, o):
            self.b_n[o].start()
            self.b_p[o].start()

        def near(self):
            self.a_n.arrived()
            self.a_fn.start()
            self.a_p.arrived()
            self.a_fp.start()
            self.cross(-1)
            self.cross(1)

        def distant(self):
            self.a_fn.arrived()
            self.a_fp.arrived()
            self.cross(2)

        def pass_on(self, o):
            self.b_n[o].arrived()
            self.b_fn[o].start()
            self.b_p[o].arrived()
            self.b_fp[o].start()

        def finish(self):
            for o in (0, -1, 1, 2):
                self.b_fn[o].arrived()
                self.b_fp[o].arrived()

    def in_piece(group):
        size = DEPTH // 2
        return (
            lambda s: win.at[rows_of(s * DEPTH + group * size, size)],
            lambda s, h: win.at[rows_of(s * DEPTH + group * size + h * (size // 2), size // 2)],
        )

    def out_piece(group):
        return (
            lambda s: wout.at[pl.ds(group * 128, 128), rows_of(s * 128, 128, 128)],
            lambda s, h: wout.at[pl.ds(group * 128 + h * 64, 64), rows_of(s * 128, 128, 128)],
        )

    ins = [Gather(g, *in_piece(g)) for g in range(2)]
    outs = [Gather(g, *out_piece(g)) for g in range(2)]
    d_out = messages.new(
        wout.at[pl.ds(0, 256)], wout.at[pl.ds(256, 256)], partner, wout.at[pl.ds(256, 256)]
    )

    pl.semaphore_wait(barrier, len(peers))

    for m in (t_n0, t_p1, t_n1, t_p0):
        m.start()
    for g in ins + outs:
        g.begin()
    d_own.start()
    for g in ins:
        g.near()
    for g in outs:
        g.near()
    for g in ins:
        g.pass_on(0)
    for g in ins:
        g.distant()
    for g in ins:
        g.pass_on(-1)
        g.pass_on(1)
    t_n0.arrived()
    f_n.start()
    d_p0.start()
    t_p1.arrived()
    f_p.start()
    d_n1.start()
    for g in outs:
        g.pass_on(0)
    for g in outs:
        g.distant()
    for g in ins:
        g.pass_on(2)
    for g in outs:
        g.pass_on(-1)
        g.pass_on(1)
    t_n1.arrived()
    d_p1.start()
    t_p0.arrived()
    d_n0.start()
    for g in ins:
        g.finish()
    for g in outs:
        g.pass_on(2)

    def spread(kv, rows, at):
        first = lax.broadcasted_iota(jnp.int32, (rows, 128), 1) < HEAD_DIM
        turned = pltpu.roll(kv, HEAD_DIM, 1)
        kp0[at, :] = jnp.where(first, kv, 0.0).astype(BF16)
        kp1[at, :] = jnp.where(first, 0.0, turned).astype(BF16)
        vp0[at, :] = jnp.where(first, turned, 0.0).astype(BF16)
        vp1[at, :] = jnp.where(first, 0.0, kv).astype(BF16)

    def project(yy):
        at = rows_of(yy * CHUNK, CHUNK)
        got = jnp.dot(tok[at, :], win[...], preferred_element_type=F32)
        qbuf[at, :] = got[:, :128].astype(BF16)
        ahead = rows_of(yy * CHUNK + WINDOW, CHUNK)
        spread(got[:, 128:256].astype(BF16).astype(F32), CHUNK, ahead)
        pool = got[:, 256:].astype(BF16)
        pext[ahead, :] = pool
        return jnp.sum(pool.astype(F32).reshape(CHUNK // 8, 8, 128), axis=0)

    d_own.arrived()
    total = project(y)
    d_p0.arrived()
    d_p1.arrived()
    total = total + project(yp)
    d_n0.arrived()
    d_n1.arrived()
    total = total + project(yn)
    f_n.arrived()
    d_f0.start()
    f_p.arrived()
    d_f1.start()
    d_f0.arrived()
    d_f1.arrived()
    total = total + project(yf)
    for g in outs:
        g.finish()
    d_out.start()

    last = pl.ds(ROWS, WINDOW)
    kvsend[...] = kp0[last, :] + vp1[last, :]
    after = (lax.rem(sp + 1, PLANE), tp)
    h_kv = messages.new(kvsend, kvland, after, kvland)
    h_p = messages.new(pext.at[last], pext.at[pl.ds(0, WINDOW)], after, pext.at[pl.ds(0, WINDOW)])
    h_kv.start()
    h_p.start()
    tot[...] = total
    sums = []
    for step in range(1, PLANE):
        m = messages.new(
            tot,
            tots.at[sp],
            (lax.rem(sp + step, PLANE), tp),
            tots.at[lax.rem(sp + PLANE - step, PLANE)],
        )
        m.start()
        sums.append(m)
    tots[sp] = total

    q_index = lax.broadcasted_iota(jnp.int32, (WINDOW, 2 * WINDOW), 0)
    k_index = lax.broadcasted_iota(jnp.int32, (WINDOW, 2 * WINDOW), 1)
    distance = q_index + WINDOW - k_index
    reach = jnp.where(y == 0, 8, jnp.where(y == 1, 32, jnp.where(y == 2, WINDOW, 1 << 24)))
    inside = (distance >= 0) & (distance < WINDOW)
    banded = (distance >= 0) & (distance < reach) & ((k_index >= WINDOW) | (y < 3))
    sinks = (sink_ref[0], sink_ref[1])

    def probabilities(q, keys, allowed, sink):
        scores = lax.dot_general(q, keys, (((1,), (1,)), ((), ())), preferred_element_type=F32)
        scores = jnp.where(allowed, scores * HEAD_DIM ** (-0.5), -jnp.inf)
        peak = jnp.maximum(jnp.max(scores, axis=1, keepdims=True), sink)
        expo = jnp.exp(scores - peak)
        denom = jnp.sum(expo, axis=1, keepdims=True) + jnp.exp(sink - peak)
        return (expo * (1.0 / denom)).astype(BF16)

    def attend(b):
        at, pair = pl.ds(b * WINDOW, WINDOW), pl.ds(b * WINDOW, 2 * WINDOW)
        allowed, band = inside, banded
        if b == 0:
            present = (k_index >= WINDOW) | (sp > 0)
            allowed, band = allowed & present, band & present
        q = qbuf[at, :]
        p0 = probabilities(q, kp0[pair, :], allowed, sinks[0])
        p1 = probabilities(q, kp1[pair, :], allowed, sinks[1])
        mixed = jnp.dot(p0, vp0[pair, :], preferred_element_type=F32)
        mixed = mixed + jnp.dot(p1, vp1[pair, :], preferred_element_type=F32)
        amine[at, pl.ds(0, 128)] = mixed.astype(BF16)
        ones = jnp.where(band, 1.0, 0.0).astype(BF16)
        sraw[at, :] = jnp.dot(ones, pext[pair, :], preferred_element_type=F32)

    for b in range(1, ROWS // WINDOW):
        attend(b)
    h_kv.arrived()
    h_p.arrived()
    spread(kvland[...].astype(F32), WINDOW, pl.ds(0, WINDOW))
    attend(0)

    for m in sums:
        m.arrived()
    earlier = lax.broadcasted_iota(jnp.int32, (PLANE, 8, 128), 0) < sp
    before = jnp.sum(jnp.sum(jnp.where(earlier, tots[...], 0.0), axis=0), axis=0, keepdims=True)
    carry = jnp.where(y == 3, before, 0.0)
    pool_gain = pgain[...]
    for b in range(ROWS // WINDOW):
        at = pl.ds(b * WINDOW, WINDOW)
        position = sp * ROWS + b * WINDOW + lax.broadcasted_iota(jnp.int32, (WINDOW, 128), 0)
        count = jnp.minimum(position + 1, reach).astype(F32)
        here = sraw[at, :]
        value = pext[pl.ds((b + 1) * WINDOW, WINDOW), :].astype(F32)
        amine[at, pl.ds(128, 128)] = (((here + carry) / count - value) * pool_gain).astype(BF16)
        carry = carry + jnp.where(y == 3, here[WINDOW - 1 :, :], 0.0)

    swaps = []
    for yy in (yf, yn, yp, y):
        src = amine.at[rows_of((yy * 2 + other) * BLOCK, BLOCK)]
        dst = apart.at[rows_of(yy * BLOCK, BLOCK)]
        m = messages.new(src, dst, partner, dst)
        m.start()
        swaps.append(m)
    d_out.arrived()

    def product(yy, put):
        mine = amine[rows_of((yy * 2 + c) * BLOCK, BLOCK), :]
        theirs = apart[rows_of(yy * BLOCK, BLOCK), :]
        for n in range(0, D, 512):
            cols = pl.ds(n, 512)
            got = jnp.dot(mine, wout[pl.ds(0, 256), cols], preferred_element_type=F32)
            got = got + jnp.dot(theirs, wout[pl.ds(256, 256), cols], preferred_element_type=F32)
            put(cols, got)

    top, bottom = pl.ds(0, HALF), pl.ds(HALF, HALF)
    r_fn = messages.new(far.at[top], rfn, up, rfn)
    r_fp = messages.new(far.at[bottom], rfp, down, rfp)
    r_n1 = messages.new(nbn.at[bottom], rn.at[bottom], up, rn.at[bottom])
    r_p0 = messages.new(nbp.at[top], rp.at[top], down, rp.at[top])
    r_n0 = messages.new(nbn.at[top], rn.at[top], up, rn.at[top])
    r_p1 = messages.new(nbp.at[bottom], rp.at[bottom], down, rp.at[bottom])

    def put_far(cols, got):
        far[:, cols] = got.astype(BF16)

    def put_next(cols, got):
        nbn[bottom, cols] = got[HALF:].astype(BF16)
        accn[:, cols] = got[:HALF]

    def put_prev(cols, got):
        nbp[top, cols] = got[:HALF].astype(BF16)
        accp[:, cols] = got[HALF:]

    swaps[0].arrived()
    product(yf, put_far)
    r_fn.start()
    r_fp.start()
    swaps[1].arrived()
    product(yn, put_next)
    r_n1.start()
    swaps[2].arrived()
    product(yp, put_prev)
    r_p0.start()
    r_fn.arrived()
    nbn[top, :] = (accn[...] + rfn[...].astype(F32)).astype(BF16)
    r_n0.start()
    r_fp.arrived()
    nbp[bottom, :] = (accp[...] + rfp[...].astype(F32)).astype(BF16)
    r_p1.start()

    swaps[3].arrived()

    def put_own(cols, got):
        accn[:, cols] = got[:HALF]
        accp[:, cols] = got[HALF:]

    product(y, put_own)
    r_n1.arrived()
    accp[...] = accp[...] + rn[bottom, :].astype(F32)
    r_p0.arrived()
    accn[...] = accn[...] + rp[top, :].astype(F32)
    r_n0.arrived()
    out_ref[top, :] = (accn[...] + rn[top, :].astype(F32)).astype(BF16)
    r_p1.arrived()
    out_ref[bottom, :] = (accp[...] + rp[bottom, :].astype(F32)).astype(BF16)
    for m in messages.made:
        m.sent()
    assert len(messages.made) <= N_MSG


def local(
    tokens_in,
    norm_gain,
    query_weight,
    key_weight,
    value_weight,
    pool_weight,
    sink_logit,
    pool_gain,
    attention_out_weight,
    pool_out_weight,
):
    hbm = pl.BlockSpec(memory_space=pltpu.HBM)
    scratch = [
        ((BLOCK, D), BF16),
        ((1, D), F32),
        ((1, 128), F32),
        ((DEPTH, DEPTH), BF16),
        ((ROWS, D), BF16),
        ((D, IN_COLS), BF16),
        ((512, D), BF16),
        ((ROWS, 128), BF16),
        ((WINDOW, 128), BF16),
        ((WINDOW, 128), BF16),
        ((ROWS + WINDOW, 128), BF16),
        ((ROWS + WINDOW, 128), BF16),
        ((ROWS + WINDOW, 128), BF16),
        ((ROWS + WINDOW, 128), BF16),
        ((ROWS + WINDOW, 128), BF16),
        ((8, 128), F32),
        ((PLANE, 8, 128), F32),
        ((ROWS, 128), F32),
        ((ROWS, 256), BF16),
        ((SIDE * BLOCK, 256), BF16),
        ((BLOCK, D), BF16),
        ((BLOCK, D), BF16),
        ((BLOCK, D), BF16),
        ((HALF, D), F32),
        ((HALF, D), F32),
        ((HALF, D), BF16),
        ((HALF, D), BF16),
        ((BLOCK, D), BF16),
        ((BLOCK, D), BF16),
    ]
    return pl.pallas_call(
        kernel,
        out_shape=jax.ShapeDtypeStruct((BLOCK, D), BF16),
        in_specs=[hbm] * 6 + [pl.BlockSpec(memory_space=pltpu.SMEM)] + [hbm] * 3,
        out_specs=pl.BlockSpec(memory_space=pltpu.VMEM),
        scratch_shapes=[pltpu.VMEM(shape, kind) for shape, kind in scratch]
        + [
            pltpu.SemaphoreType.DMA((9,)),
            pltpu.SemaphoreType.DMA((N_MSG,)),
            pltpu.SemaphoreType.DMA((N_MSG,)),
        ],
        compiler_params=pltpu.CompilerParams(
            collective_id=0, has_side_effects=True, vmem_limit_bytes=62 * 1024 * 1024
        ),
    )(
        tokens_in,
        norm_gain.reshape(1, D),
        query_weight,
        key_weight.T,
        value_weight.T,
        pool_weight,
        sink_logit,
        pool_gain.reshape(1, 128),
        attention_out_weight,
        pool_out_weight,
    )


def solution(mesh):
    in_specs = (
        P(("sp", "tp"), None),
        P(),
        P("sp", "tp"),
        P("sp", "tp"),
        P("sp", "tp"),
        P("sp", "tp"),
        P("tp"),
        P("tp"),
        P("tp", "sp"),
        P("tp", "sp"),
    )
    out_specs = P(("sp", "tp"), None)
    return jax.shard_map(local, mesh=mesh, in_specs=in_specs, out_specs=out_specs, check_vma=False)
```

```python
import jax
import jax.numpy as jnp
from jax import lax
from jax.experimental import pallas as pl
from jax.experimental.pallas import tpu as pltpu
from jax.sharding import PartitionSpec as P

MESH = pl.DeviceIdType.MESH
F32 = jnp.float32
BF16 = jnp.bfloat16

D = 2048
HEAD_DIM = 64
WINDOW = 128
EPS = 1e-06
SIDE = 4
PLANE = SIDE * SIDE
BLOCK = 96
HALF = BLOCK // 2
ROWS = 2 * SIDE * BLOCK
CHUNK = 2 * BLOCK
DEPTH = D // PLANE
IN_COLS = 384
N_GROUPS = 40


class Groups:
    def __init__(self, send_sems, recv_sems):
        self.send_sems, self.recv_sems, self.made = send_sems, recv_sems, []

    def new(self, whole):
        group = Group(self.send_sems.at[len(self.made)], self.recv_sems.at[len(self.made)], whole)
        self.made.append(group)
        return group

    def one(self, src, dst, device, land):
        group = self.new(land)
        group.add(src, dst, device)
        return group


class Group:
    def __init__(self, send_sem, recv_sem, whole):
        self.send_sem, self.recv_sem, self.whole, self.copies = send_sem, recv_sem, whole, []

    def copy(self, src, dst, device):
        return pltpu.make_async_remote_copy(
            src_ref=src,
            dst_ref=dst,
            send_sem=self.send_sem,
            recv_sem=self.recv_sem,
            device_id=device,
            device_id_type=MESH,
        )

    def add(self, src, dst, device):
        self.device = device
        self.copies.append((src, dst, device))
        return len(self.copies) - 1

    def start(self, *which):
        for n in which or range(len(self.copies)):
            self.copy(*self.copies[n]).start()

    def arrived(self):
        self.copy(self.whole, self.whole, self.device).wait_recv()

    def sent(self):
        self.copy(self.whole, self.whole, self.device).wait_send()


def rows_of(start, size, unit=16):
    return pl.ds(pl.multiple_of(start, unit), size)


def kernel(
    x_hbm,
    gain_hbm,
    wq_hbm,
    wk_hbm,
    wv_hbm,
    wp_hbm,
    sink_hbm,
    pgain_hbm,
    wa_hbm,
    wo_hbm,
    out_ref,
    xin,
    gain,
    pgain,
    sink,
    wkv,
    tok,
    win,
    wout,
    qbuf,
    kvsend,
    kvland,
    kp0,
    kp1,
    vp0,
    vp1,
    pext,
    totals,
    before,
    cols_own,
    cols_y,
    cols_core,
    cols_other,
    cols_sp,
    amine,
    apart,
    far,
    nbn,
    nbp,
    accn,
    accp,
    rfn,
    rfp,
    rn,
    rp,
    local_sems,
    send_sems,
    recv_sems,
):
    sp = lax.axis_index("sp")
    tp = lax.axis_index("tp")
    z, x = sp // SIDE, lax.rem(sp, SIDE)
    y, c = tp // 2, lax.rem(tp, 2)
    other = 1 - c

    def turn(i, by):
        return lax.rem(i + by + SIDE, SIDE)

    yn, yp, yf = turn(y, 1), turn(y, -1), turn(y, 2)
    partner = (sp, y * 2 + other)
    up, down = (sp, yn * 2 + c), (sp, yp * 2 + c)

    barrier = pltpu.get_barrier_semaphore()
    beside = [(z * SIDE + turn(x, by), tp) for by in (1, -1)]
    above = [(turn(z, by) * SIDE + x, tp) for by in (1, -1)]
    opposite = [(z * SIDE + turn(x, 2), tp), (turn(z, 2) * SIDE + x, tp), (sp, yf * 2 + c)]
    peers = [up, down, partner] + beside + above + opposite
    for peer in peers:
        pl.semaphore_signal(barrier, inc=1, device_id=peer, device_id_type=MESH)

    own_in = rows_of(sp * DEPTH, DEPTH, 128)
    own_cols = rows_of(sp * 128, 128, 128)
    loads = [
        (0, x_hbm, xin),
        (1, gain_hbm, gain),
        (2, wk_hbm, wkv.at[pl.ds(0, HEAD_DIM)]),
        (2, wv_hbm, wkv.at[pl.ds(HEAD_DIM, HEAD_DIM)]),
        (3, wq_hbm, win.at[own_in, pl.ds(0, 128)]),
        (3, wp_hbm, win.at[own_in, pl.ds(256, 128)]),
        (4, wa_hbm, wout.at[pl.ds(0, 128), own_cols]),
        (4, wo_hbm, wout.at[pl.ds(128, 128), own_cols]),
        (5, pgain_hbm, pgain),
        (6, sink_hbm, sink),
    ]
    for n, src, dst in loads:
        pltpu.make_async_copy(src, dst, local_sems.at[n]).start()

    def loaded(n, whole):
        pltpu.make_async_copy(whole, whole, local_sems.at[n]).wait()

    loaded(0, xin)
    loaded(1, gain)
    gains = gain[...]

    def column_sums(rows):
        return jnp.sum(rows.astype(F32), axis=0, keepdims=True)

    columns = jnp.zeros((1, D), F32)
    for r in range(0, BLOCK, 16):
        wide = xin[pl.ds(r, 16)].astype(F32)
        inverse = lax.rsqrt(jnp.mean(wide * wide, axis=1, keepdims=True) + EPS)
        normed = (wide * inverse * gains).astype(BF16)
        tok[rows_of(tp * BLOCK + r, 16), :] = normed
        columns = columns + column_sums(normed)
    cols_own[...] = columns
    loaded(2, wkv)
    win[own_in, pl.ds(128, 128)] = wkv[...].T
    loaded(3, win.at[own_in, pl.ds(0, 256)])
    loaded(4, wout.at[pl.ds(0, 256), own_cols])
    loaded(5, pgain)
    loaded(6, sink)

    groups = Groups(send_sems, recv_sems)

    def block(yy, cc):
        return tok.at[rows_of((yy * 2 + cc) * BLOCK, BLOCK)]

    def half(yy, cc, h):
        return tok.at[rows_of((yy * 2 + cc) * BLOCK + h * HALF, HALF)]

    one = groups.one
    c_y = groups.new(cols_y)
    for n, by in enumerate((1, -1, 2)):
        c_y.add(cols_own, cols_y.at[n], (sp, turn(y, by) * 2 + c))
    t_n0 = one(half(y, c, 0), half(y, c, 0), up, half(yp, c, 0))
    t_p1 = one(half(y, c, 1), half(y, c, 1), down, half(yn, c, 1))
    t_n1 = one(half(y, c, 1), half(y, c, 1), up, half(yp, c, 1))
    t_p0 = one(half(y, c, 0), half(y, c, 0), down, half(yn, c, 0))
    f_n = one(half(yp, c, 0), half(yp, c, 0), up, half(yf, c, 0))
    f_p = one(half(yn, c, 1), half(yn, c, 1), down, half(yf, c, 1))
    d_own = one(block(y, c), block(y, c), partner, block(y, other))

    def across(yy):
        group = groups.new(block(yy, other))
        for h in range(2):
            group.add(half(yy, c, h), half(yy, c, h), partner)
        return group

    d_p, d_n, d_f = across(yp), across(yn), across(yf)
    c_core = one(cols_core, cols_other, partner, cols_other)
    c_sp = groups.new(cols_sp.at[pl.ds(0, PLANE - 1)])
    for step in range(1, PLANE):
        c_sp.add(cols_sp.at[sp], cols_sp.at[sp], (lax.rem(sp + step, PLANE), tp))

    class Gather:
        def __init__(self, piece, sub, whole, direct, crossing_direct, shared=None):
            def source(g, o1, o2):
                if g == 0:
                    return turn(z, o2) * SIDE + turn(x, o1)
                return turn(z, o1) * SIDE + turn(x, o2)

            def put(group, ref, g, o1, o2):
                return group.add(ref, ref, (source(g, o1, o2), tp))

            self.first = groups.new(whole(4))
            self.first_far = groups.new(whole(2))
            self.last = groups.new(whole(8))
            self.direct = direct
            self.second, self.forward = {}, {}
            for g in range(2):
                mine = piece(g, source(g, 0, 0))
                put(self.first, mine, g, 1, 0)
                put(self.first, mine, g, -1, 0)
                if direct:
                    put(self.first_far, mine, g, 2, 0)
                else:
                    put(self.first_far, sub(g, source(g, -1, 0), 0), g, 1, 0)
                    put(self.first_far, sub(g, source(g, 1, 0), 1), g, -1, 0)
            for o in (0, -1, 1, 2):
                self.second[o] = groups.new(whole(4))
                self.forward[o] = []
                for g in range(2):
                    have = piece(g, source(g, o, 0))
                    put(self.second[o], have, g, 0, 1)
                    put(self.second[o], have, g, 0, -1)
                    if o in crossing_direct:
                        self.forward[o].append(put(self.last, have, g, 0, 2))
                    else:
                        low, high = sub(g, source(g, o, -1), 0), sub(g, source(g, o, 1), 1)
                        self.forward[o].append(put(self.last, low, g, 0, 1))
                        self.forward[o].append(put(self.last, high, g, 0, -1))
            self.crossing_direct = crossing_direct
            self.shares = None
            if shared:
                self.shares = groups.new(shared[0])
                self.share_of = {}
                for o1 in (0, -1, 1, 2):
                    for o2 in (0, -1, 1, 2):
                        self.share_of[o1, o2] = [
                            self.shares.add(
                                piece(g, source(g, o1, o2)), shared[1](g, source(g, o1, o2)), partner
                            )
                            for g in range(2)
                        ]

        def share(self, o1, o2):
            if self.shares:
                self.shares.start(*self.share_of[o1, o2])

        def begin(self):
            self.first.start()
            if self.direct:
                self.first_far.start()

        def cross(self, o):
            self.second[o].start()
            if o in self.crossing_direct:
                self.last.start(*self.forward[o])
            self.share(o, 0)

        def near(self):
            self.first.arrived()
            if not self.direct:
                self.first_far.start()
            self.cross(-1)
            self.cross(1)

        def distant(self):
            self.first_far.arrived()
            self.cross(2)

        def pass_on(self, o):
            self.second[o].arrived()
            if o not in self.crossing_direct:
                self.last.start(*self.forward[o])
            self.share(o, -1)
            self.share(o, 1)

        def finish(self):
            self.last.arrived()
            for o in (0, -1, 1, 2):
                self.share(o, 2)

    size = DEPTH // 2
    ins = Gather(
        lambda g, s: win.at[rows_of(s * DEPTH + g * size, size)],
        lambda g, s, h: win.at[rows_of(s * DEPTH + g * size + h * (size // 2), size // 2)],
        lambda n: win.at[pl.ds(0, n * size)],
        True,
        (),
    )
    outs = Gather(
        lambda g, s: wout.at[pl.ds(g * 128, 128), rows_of(s * 128, 128, 128)],
        lambda g, s, h: wout.at[pl.ds(g * 128 + h * 64, 64), rows_of(s * 128, 128, 128)],
        lambda n: wout.at[pl.ds(0, n * 8)],
        False,
        (2,),
        (
            wout.at[pl.ds(256, 256)],
            lambda g, s: wout.at[pl.ds(256 + g * 128, 128), rows_of(s * 128, 128, 128)],
        ),
    )

    pl.semaphore_wait(barrier, len(peers))

    for group in (c_y, t_n0, t_p1, t_n1, t_p0):
        group.start()
    ins.begin()
    outs.begin()
    ins.cross(0)
    outs.cross(0)
    d_own.start()
    ins.near()
    ins.distant()
    c_y.arrived()
    own_parity = columns + cols_y[0] + cols_y[1] + cols_y[2]
    cols_core[...] = own_parity
    c_core.start()
    outs.near()
    ins.pass_on(0)
    c_core.arrived()
    cols_sp[sp] = own_parity + cols_other[...]

    @pl.when(y == SIDE - 1)
    def _():
        c_sp.start()

    t_n0.arrived()
    f_n.start()
    d_p.start(0)
    t_p1.arrived()
    f_p.start()
    d_n.start(1)
    outs.pass_on(0)
    ins.pass_on(-1)
    ins.pass_on(1)
    ins.pass_on(2)
    outs.distant()
    t_n1.arrived()
    d_p.start(1)
    t_p0.arrived()
    d_n.start(0)
    outs.pass_on(-1)
    outs.pass_on(1)
    ins.finish()

    def spread(kv, rows, at):
        first = lax.broadcasted_iota(jnp.int32, (rows, 128), 1) < HEAD_DIM
        turned = pltpu.roll(kv, HEAD_DIM, 1)
        kp0[at, :] = jnp.where(first, kv, 0.0).astype(BF16)
        kp1[at, :] = jnp.where(first, 0.0, turned).astype(BF16)
        vp0[at, :] = jnp.where(first, turned, 0.0).astype(BF16)
        vp1[at, :] = jnp.where(first, 0.0, kv).astype(BF16)

    last = pl.ds(ROWS, WINDOW)
    after = (lax.rem(sp + 1, PLANE), tp)
    halo = groups.new(pext.at[pl.ds(0, 2 * WINDOW)])
    halo.add(kvsend, kvland, after)
    halo.add(pext.at[last], pext.at[pl.ds(0, WINDOW)], after)

    def project(yy):
        at = rows_of(yy * CHUNK, CHUNK)
        got = jnp.dot(tok[at, :], win[...], preferred_element_type=F32)
        qbuf[at, :] = got[:, :128].astype(BF16)
        ahead = rows_of(yy * CHUNK + WINDOW, CHUNK)
        spread(got[:, 128:256].astype(BF16).astype(F32), CHUNK, ahead)
        pool = got[:, 256:].astype(BF16)
        pext[ahead, :] = pool
        sums = jnp.sum(pool.astype(F32).reshape(2, BLOCK // 8, 8, 128), axis=1)
        totals[pl.ds(yy * 2, 2)] = sums

        @pl.when(yy == SIDE - 1)
        def _():
            kvsend[...] = kp0[last, :] + vp1[last, :]
            halo.start()

    f_n.arrived()
    d_f.start(0)
    f_p.arrived()
    d_f.start(1)
    d_own.arrived()
    project(y)
    d_p.arrived()
    project(yp)
    d_n.arrived()
    project(yn)
    outs.pass_on(2)
    d_f.arrived()
    project(yf)
    outs.finish()

    @pl.when(y == SIDE - 1)
    def _():
        c_sp.arrived()
        earlier = lax.broadcasted_iota(jnp.int32, (PLANE, 1, D), 0) < sp
        ahead = jnp.sum(jnp.where(earlier, cols_sp[...], 0.0), axis=0)
        high = ahead.astype(BF16).astype(F32)
        middle = (ahead - high).astype(BF16).astype(F32)
        low = ahead - high - middle
        term = lax.broadcasted_iota(jnp.int32, (16, D), 0)
        terms = jnp.where(term == 0, high, jnp.where(term == 1, middle, jnp.where(term == 2, low, 0.0)))
        got = jnp.dot(terms.astype(BF16), win[:, 256:], preferred_element_type=F32)
        before[...] = jnp.sum(got, axis=0, keepdims=True)

    span = WINDOW + BLOCK
    q_index = lax.broadcasted_iota(jnp.int32, (BLOCK, span), 0)
    k_index = lax.broadcasted_iota(jnp.int32, (BLOCK, span), 1)
    distance = q_index + WINDOW - k_index
    reach = jnp.where(y == 0, 8, jnp.where(y == 1, 32, jnp.where(y == 2, WINDOW, 1 << 24)))
    inside = (distance >= 0) & (distance < WINDOW)
    banded = (distance >= 0) & (distance < reach) & ((k_index >= WINDOW) | (y < 3))
    sinks = (sink[:, 0:1], sink[:, 1:2])
    pool_gain = pgain[...]

    def probabilities(q, keys, allowed, sink):
        scores = lax.dot_general(q, keys, (((1,), (1,)), ((), ())), preferred_element_type=F32)
        scores = jnp.where(allowed, scores * HEAD_DIM ** (-0.5), -jnp.inf)
        peak = jnp.maximum(jnp.max(scores, axis=1, keepdims=True), sink)
        expo = jnp.exp(scores - peak)
        denom = jnp.sum(expo, axis=1, keepdims=True) + jnp.exp(sink - peak)
        return (expo * (1.0 / denom)).astype(BF16)

    def attend(yy, cc):
        number = yy * 2 + cc
        start = sp * ROWS + number * BLOCK
        at, pair = rows_of(number * BLOCK, BLOCK), rows_of(number * BLOCK, span)
        present = k_index >= WINDOW - start
        allowed, band = inside & present, banded & present
        q = qbuf[at, :]
        p0 = probabilities(q, kp0[pair, :], allowed, sinks[0])
        p1 = probabilities(q, kp1[pair, :], allowed, sinks[1])
        mixed = jnp.dot(p0, vp0[pair, :], preferred_element_type=F32)
        mixed = mixed + jnp.dot(p1, vp1[pair, :], preferred_element_type=F32)
        amine[at, pl.ds(0, 128)] = mixed.astype(BF16)
        ones = jnp.where(band, 1.0, 0.0).astype(BF16)
        sums = jnp.dot(ones, pext[pair, :], preferred_element_type=F32)
        earlier = lax.broadcasted_iota(jnp.int32, (2 * SIDE, 8, 128), 0) < number
        carry = jnp.sum(jnp.sum(jnp.where(earlier, totals[...], 0.0), axis=0), axis=0, keepdims=True)
        carry = jnp.where(y == 3, carry + before[...], 0.0)
        position = start + lax.broadcasted_iota(jnp.int32, (BLOCK, 128), 0)
        count = jnp.minimum(position + 1, reach).astype(F32)
        value = pext[rows_of(number * BLOCK + WINDOW, BLOCK), :].astype(F32)
        pooled = (sums + carry) / count
        amine[at, pl.ds(128, 128)] = ((pooled - value) * pool_gain).astype(BF16)

    def first_half(yy):
        @pl.when(yy == 0)
        def _():
            halo.arrived()
            spread(kvland[...].astype(F32), WINDOW, pl.ds(0, WINDOW))

        attend(yy, other)
        src = amine.at[rows_of((yy * 2 + other) * BLOCK, BLOCK)]
        dst = apart.at[rows_of(yy * BLOCK, BLOCK)]
        swap = one(src, dst, partner, dst)
        swap.start()
        return swap

    def product(yy, put):
        mine = amine[rows_of((yy * 2 + c) * BLOCK, BLOCK), :]
        theirs = apart[rows_of(yy * BLOCK, BLOCK), :]
        for n in range(0, D, 512):
            cols = pl.ds(n, 512)
            got = jnp.dot(mine, wout[pl.ds(0, 256), cols], preferred_element_type=F32)
            got = got + jnp.dot(theirs, wout[pl.ds(256, 256), cols], preferred_element_type=F32)
            put(cols, got)

    top, bottom = pl.ds(0, HALF), pl.ds(HALF, HALF)
    r_fn = one(far.at[top], rfn, up, rfn)
    r_fp = one(far.at[bottom], rfp, down, rfp)
    r_n1 = one(nbn.at[bottom], rn.at[bottom], up, rn.at[bottom])
    r_p0 = one(nbp.at[top], rp.at[top], down, rp.at[top])
    r_n0 = one(nbn.at[top], rn.at[top], up, rn.at[top])
    r_p1 = one(nbp.at[bottom], rp.at[bottom], down, rp.at[bottom])

    def put_far(cols, got):
        far[:, cols] = got.astype(BF16)

    def put_next(cols, got):
        nbn[bottom, cols] = got[HALF:].astype(BF16)
        accn[:, cols] = got[:HALF]

    def put_prev(cols, got):
        nbp[top, cols] = got[:HALF].astype(BF16)
        accp[:, cols] = got[HALF:]

    swap_f = first_half(yf)
    attend(yf, c)
    swap_n = first_half(yn)
    outs.shares.arrived()
    swap_f.arrived()
    product(yf, put_far)
    r_fn.start()
    r_fp.start()
    attend(yn, c)
    swap_p = first_half(yp)
    swap_n.arrived()
    product(yn, put_next)
    r_n1.start()
    attend(yp, c)
    swap_o = first_half(y)
    swap_p.arrived()
    product(yp, put_prev)
    r_p0.start()
    attend(y, c)
    r_fn.arrived()
    nbn[top, :] = (accn[...] + rfn[...].astype(F32)).astype(BF16)
    r_n0.start()
    r_fp.arrived()
    nbp[bottom, :] = (accp[...] + rfp[...].astype(F32)).astype(BF16)
    r_p1.start()
    swap_o.arrived()

    def put_own(cols, got):
        accn[:, cols] = got[:HALF]
        accp[:, cols] = got[HALF:]

    product(y, put_own)
    r_n1.arrived()
    accp[...] = accp[...] + rn[bottom, :].astype(F32)
    r_p0.arrived()
    accn[...] = accn[...] + rp[top, :].astype(F32)
    r_n0.arrived()
    out_ref[top, :] = (accn[...] + rn[top, :].astype(F32)).astype(BF16)
    r_p1.arrived()
    out_ref[bottom, :] = (accp[...] + rp[bottom, :].astype(F32)).astype(BF16)
    for group in groups.made:
        if group is not c_sp:
            group.sent()

    @pl.when(y == SIDE - 1)
    def _():
        c_sp.sent()

    assert len(groups.made) <= N_GROUPS


def local(
    tokens_in,
    norm_gain,
    query_weight,
    key_weight,
    value_weight,
    pool_weight,
    sink_logit,
    pool_gain,
    attention_out_weight,
    pool_out_weight,
):
    hbm = pl.BlockSpec(memory_space=pltpu.HBM)
    scratch = [
        ((BLOCK, D), BF16),
        ((1, D), F32),
        ((1, 128), F32),
        ((1, 2), F32),
        ((DEPTH, DEPTH), BF16),
        ((ROWS, D), BF16),
        ((D, IN_COLS), BF16),
        ((512, D), BF16),
        ((ROWS, 128), BF16),
        ((WINDOW, 128), BF16),
        ((WINDOW, 128), BF16),
        ((ROWS + WINDOW, 128), BF16),
        ((ROWS + WINDOW, 128), BF16),
        ((ROWS + WINDOW, 128), BF16),
        ((ROWS + WINDOW, 128), BF16),
        ((ROWS + WINDOW, 128), BF16),
        ((2 * SIDE, 8, 128), F32),
        ((1, 128), F32),
        ((1, D), F32),
        ((3, 1, D), F32),
        ((1, D), F32),
        ((1, D), F32),
        ((PLANE, 1, D), F32),
        ((ROWS, 256), BF16),
        ((SIDE * BLOCK, 256), BF16),
        ((BLOCK, D), BF16),
        ((BLOCK, D), BF16),
        ((BLOCK, D), BF16),
        ((HALF, D), F32),
        ((HALF, D), F32),
        ((HALF, D), BF16),
        ((HALF, D), BF16),
        ((BLOCK, D), BF16),
        ((BLOCK, D), BF16),
    ]
    return pl.pallas_call(
        kernel,
        out_shape=jax.ShapeDtypeStruct((BLOCK, D), BF16),
        in_specs=[hbm] * 10,
        out_specs=pl.BlockSpec(memory_space=pltpu.VMEM),
        scratch_shapes=[pltpu.VMEM(shape, kind) for shape, kind in scratch]
        + [
            pltpu.SemaphoreType.DMA((7,)),
            pltpu.SemaphoreType.DMA((N_GROUPS,)),
            pltpu.SemaphoreType.DMA((N_GROUPS,)),
        ],
        compiler_params=pltpu.CompilerParams(
            collective_id=0, has_side_effects=True, vmem_limit_bytes=62 * 1024 * 1024
        ),
    )(
        tokens_in,
        norm_gain.reshape(1, D),
        query_weight,
        key_weight.T,
        value_weight.T,
        pool_weight,
        sink_logit.reshape(1, 2),
        pool_gain.reshape(1, 128),
        attention_out_weight,
        pool_out_weight,
    )


def solution(mesh):
    in_specs = (
        P(("sp", "tp"), None),
        P(),
        P("sp", "tp"),
        P("sp", "tp"),
        P("sp", "tp"),
        P("sp", "tp"),
        P("tp"),
        P("tp"),
        P("tp", "sp"),
        P("tp", "sp"),
    )
    out_specs = P(("sp", "tp"), None)
    return jax.shard_map(local, mesh=mesh, in_specs=in_specs, out_specs=out_specs, check_vma=False)
```

```python
import jax
import jax.numpy as jnp
from jax import lax
from jax.experimental import pallas as pl
from jax.experimental.pallas import tpu as pltpu
from jax.sharding import PartitionSpec as P

MESH = pl.DeviceIdType.MESH
F32 = jnp.float32
BF16 = jnp.bfloat16

D = 2048
HEAD_DIM = 64
WINDOW = 128
EPS = 1e-06
SIDE = 4
PLANE = SIDE * SIDE
BLOCK = 96
HALF = BLOCK // 2
ROWS = 2 * SIDE * BLOCK
CHUNK = 2 * BLOCK
DEPTH = D // PLANE
IN_COLS = 384
N_GROUPS = 48
PART = 16
EARLY = 2


class Groups:
    def __init__(self, send_sems, recv_sems):
        self.send_sems, self.recv_sems, self.made = send_sems, recv_sems, []

    def new(self, whole):
        group = Group(self.send_sems.at[len(self.made)], self.recv_sems.at[len(self.made)], whole)
        self.made.append(group)
        return group

    def one(self, src, dst, device, land):
        group = self.new(land)
        group.add(src, dst, device)
        return group


class Group:
    def __init__(self, send_sem, recv_sem, whole):
        self.send_sem, self.recv_sem, self.whole, self.copies = send_sem, recv_sem, whole, []

    def copy(self, src, dst, device):
        return pltpu.make_async_remote_copy(
            src_ref=src,
            dst_ref=dst,
            send_sem=self.send_sem,
            recv_sem=self.recv_sem,
            device_id=device,
            device_id_type=MESH,
        )

    def add(self, src, dst, device):
        self.device = device
        self.copies.append((src, dst, device))
        return len(self.copies) - 1

    def start(self, *which):
        for n in which or range(len(self.copies)):
            self.copy(*self.copies[n]).start()

    def arrived(self):
        self.copy(self.whole, self.whole, self.device).wait_recv()

    def sent(self):
        self.copy(self.whole, self.whole, self.device).wait_send()


def rows_of(start, size, unit=16):
    return pl.ds(pl.multiple_of(start, unit), size)


def kernel(
    x_hbm,
    gain_hbm,
    wq_hbm,
    wk_hbm,
    wv_hbm,
    wp_hbm,
    sink_hbm,
    pgain_hbm,
    wa_hbm,
    wo_hbm,
    out_hbm,
    xin,
    gain,
    pgain,
    sink,
    wkv,
    tok,
    win,
    wout,
    qbuf,
    kvsend,
    kvland,
    kp0,
    kp1,
    vp0,
    vp1,
    pext,
    totals,
    before,
    cols_own,
    cols_y,
    cols_core,
    cols_other,
    cols_chip,
    cols_row,
    cols_x,
    cols_z,
    terms,
    amine,
    apart,
    exact,
    rounded,
    from_prev,
    from_next,
    result,
    local_sems,
    out_sems,
    send_sems,
    recv_sems,
):
    sp = lax.axis_index("sp")
    tp = lax.axis_index("tp")
    z, x = sp // SIDE, lax.rem(sp, SIDE)
    y, c = tp // 2, lax.rem(tp, 2)
    other = 1 - c

    def turn(i, by):
        return lax.rem(i + by + SIDE, SIDE)

    yn, yp, yf = turn(y, 1), turn(y, -1), turn(y, 2)
    partner = (sp, y * 2 + other)
    up, down = (sp, yn * 2 + c), (sp, yp * 2 + c)

    barrier = pltpu.get_barrier_semaphore()
    beside = [(z * SIDE + turn(x, by), tp) for by in (1, -1)]
    above = [(turn(z, by) * SIDE + x, tp) for by in (1, -1)]
    opposite = [(z * SIDE + turn(x, 2), tp), (turn(z, 2) * SIDE + x, tp), (sp, yf * 2 + c)]
    peers = [up, down, partner] + beside + above + opposite
    for peer in peers:
        pl.semaphore_signal(barrier, inc=1, device_id=peer, device_id_type=MESH)

    own_in = rows_of(sp * DEPTH, DEPTH, 128)
    own_cols = rows_of(sp * 128, 128, 128)
    loads = [
        (0, x_hbm, xin),
        (1, gain_hbm, gain),
        (2, wk_hbm, wkv.at[pl.ds(0, HEAD_DIM)]),
        (2, wv_hbm, wkv.at[pl.ds(HEAD_DIM, HEAD_DIM)]),
        (3, wq_hbm, win.at[own_in, pl.ds(0, 128)]),
        (3, wp_hbm, win.at[own_in, pl.ds(256, 128)]),
        (4, wa_hbm, wout.at[pl.ds(0, 128), own_cols]),
        (4, wo_hbm, wout.at[pl.ds(128, 128), own_cols]),
        (5, pgain_hbm, pgain),
        (6, sink_hbm, sink),
    ]
    for n, src, dst in loads:
        pltpu.make_async_copy(src, dst, local_sems.at[n]).start()

    def loaded(n, whole):
        pltpu.make_async_copy(whole, whole, local_sems.at[n]).wait()

    loaded(0, xin)
    loaded(1, gain)
    gains = gain[...]

    def column_sums(rows):
        return jnp.sum(rows.astype(F32), axis=0, keepdims=True)

    columns = jnp.zeros((1, D), F32)
    for r in range(0, BLOCK, 16):
        wide = xin[pl.ds(r, 16)].astype(F32)
        inverse = lax.rsqrt(jnp.mean(wide * wide, axis=1, keepdims=True) + EPS)
        normed = (wide * inverse * gains).astype(BF16)
        tok[rows_of(tp * BLOCK + r, 16), :] = normed
        columns = columns + column_sums(normed)
    cols_own[...] = columns
    loaded(2, wkv)
    win[own_in, pl.ds(128, 128)] = wkv[...].T
    loaded(3, win.at[own_in, pl.ds(0, 256)])
    loaded(4, wout.at[pl.ds(0, 256), own_cols])
    loaded(5, pgain)
    loaded(6, sink)

    groups = Groups(send_sems, recv_sems)

    def block(yy, cc):
        return tok.at[rows_of((yy * 2 + cc) * BLOCK, BLOCK)]

    def half(yy, cc, h):
        return tok.at[rows_of((yy * 2 + cc) * BLOCK + h * HALF, HALF)]

    one = groups.one
    c_y = groups.new(cols_y)
    for n, by in enumerate((1, -1, 2)):
        c_y.add(cols_own, cols_y.at[n], (sp, turn(y, by) * 2 + c))
    t_n0 = one(half(y, c, 0), half(y, c, 0), up, half(yp, c, 0))
    t_p1 = one(half(y, c, 1), half(y, c, 1), down, half(yn, c, 1))
    t_n1 = one(half(y, c, 1), half(y, c, 1), up, half(yp, c, 1))
    t_p0 = one(half(y, c, 0), half(y, c, 0), down, half(yn, c, 0))
    f_n = one(half(yp, c, 0), half(yp, c, 0), up, half(yf, c, 0))
    f_p = one(half(yn, c, 1), half(yn, c, 1), down, half(yf, c, 1))
    d_own = one(block(y, c), block(y, c), partner, block(y, other))

    def across(yy):
        group = groups.new(block(yy, other))
        for h in range(2):
            group.add(half(yy, c, h), half(yy, c, h), partner)
        return group

    d_p, d_n, d_f = across(yp), across(yn), across(yf)
    c_core = one(cols_core, cols_other, partner, cols_other)
    c_x, c_z = groups.new(cols_x), groups.new(cols_z)
    for n, by in enumerate((1, -1, 2)):
        c_x.add(cols_chip, cols_x.at[n], (z * SIDE + turn(x, by), tp))
        c_z.add(cols_row, cols_z.at[n], (turn(z, by) * SIDE + x, tp))
    prefix_groups = (c_x, c_z)

    def summed(own, slots, here=None):
        total = own
        for n, by in enumerate((-1, 1, 2)):
            if here is None:
                total = total + slots[n]
            else:
                total = total + jnp.where(turn(here, by) < here, slots[n], 0.0)
        return total

    class Gather:
        def __init__(self, piece, sub, whole, direct, crossing_direct, shared=None):
            def source(g, o1, o2):
                if g == 0:
                    return turn(z, o2) * SIDE + turn(x, o1)
                return turn(z, o1) * SIDE + turn(x, o2)

            def put(group, ref, g, o1, o2):
                return group.add(ref, ref, (source(g, o1, o2), tp))

            self.first = groups.new(whole(4))
            self.first_far = groups.new(whole(2))
            self.last = groups.new(whole(8))
            self.direct = direct
            self.second, self.forward = {}, {}
            for g in range(2):
                mine = piece(g, source(g, 0, 0))
                put(self.first, mine, g, 1, 0)
                put(self.first, mine, g, -1, 0)
                if direct:
                    put(self.first_far, mine, g, 2, 0)
                else:
                    put(self.first_far, sub(g, source(g, -1, 0), 0), g, 1, 0)
                    put(self.first_far, sub(g, source(g, 1, 0), 1), g, -1, 0)
            for o in (0, -1, 1, 2):
                self.second[o] = groups.new(whole(4))
                self.forward[o] = []
                for g in range(2):
                    have = piece(g, source(g, o, 0))
                    put(self.second[o], have, g, 0, 1)
                    put(self.second[o], have, g, 0, -1)
                    if o in crossing_direct:
                        self.forward[o].append(put(self.last, have, g, 0, 2))
                    else:
                        low, high = sub(g, source(g, o, -1), 0), sub(g, source(g, o, 1), 1)
                        self.forward[o].append(put(self.last, low, g, 0, 1))
                        self.forward[o].append(put(self.last, high, g, 0, -1))
            self.crossing_direct = crossing_direct
            self.shares = None
            if shared:
                self.shares = groups.new(shared[0])
                self.share_of = {}
                for o1 in (0, -1, 1, 2):
                    for o2 in (0, -1, 1, 2):
                        self.share_of[o1, o2] = [
                            self.shares.add(
                                piece(g, source(g, o1, o2)), shared[1](g, source(g, o1, o2)), partner
                            )
                            for g in range(2)
                        ]

        def share(self, o1, o2):
            if self.shares:
                self.shares.start(*self.share_of[o1, o2])

        def begin(self):
            self.first.start()
            if self.direct:
                self.first_far.start()

        def cross(self, o):
            self.second[o].start()
            if o in self.crossing_direct:
                self.last.start(*self.forward[o])
            self.share(o, 0)

        def near(self):
            self.first.arrived()
            if not self.direct:
                self.first_far.start()
            self.cross(-1)
            self.cross(1)

        def distant(self):
            self.first_far.arrived()
            self.cross(2)

        def pass_on(self, o):
            self.second[o].arrived()
            if o not in self.crossing_direct:
                self.last.start(*self.forward[o])
            self.share(o, -1)
            self.share(o, 1)

        def finish(self):
            self.last.arrived()
            for o in (0, -1, 1, 2):
                self.share(o, 2)

    size = DEPTH // 2
    ins = Gather(
        lambda g, s: win.at[rows_of(s * DEPTH + g * size, size)],
        lambda g, s, h: win.at[rows_of(s * DEPTH + g * size + h * (size // 2), size // 2)],
        lambda n: win.at[pl.ds(0, n * size)],
        True,
        (),
    )
    outs = Gather(
        lambda g, s: wout.at[pl.ds(g * 128, 128), rows_of(s * 128, 128, 128)],
        lambda g, s, h: wout.at[pl.ds(g * 128 + h * 64, 64), rows_of(s * 128, 128, 128)],
        lambda n: wout.at[pl.ds(0, n * 8)],
        False,
        (2,),
        (
            wout.at[pl.ds(256, 256)],
            lambda g, s: wout.at[pl.ds(256 + g * 128, 128), rows_of(s * 128, 128, 128)],
        ),
    )

    pl.semaphore_wait(barrier, len(peers))

    for group in (c_y, t_n0, t_p1, t_n1, t_p0):
        group.start()
    ins.begin()
    outs.begin()
    ins.cross(0)
    outs.cross(0)
    d_own.start()
    ins.near()
    ins.distant()
    c_y.arrived()
    own_parity = summed(columns, cols_y)
    cols_core[...] = own_parity
    c_core.start()
    outs.near()
    ins.pass_on(0)
    c_core.arrived()
    cols_chip[...] = own_parity + cols_other[...]

    @pl.when(y == SIDE - 1)
    def _():
        c_x.start()

    t_n0.arrived()
    f_n.start()
    d_p.start(0)
    t_p1.arrived()
    f_p.start()
    d_n.start(1)
    outs.pass_on(0)
    ins.pass_on(-1)
    ins.pass_on(1)
    ins.pass_on(2)
    outs.distant()

    t_n1.arrived()
    d_p.start(1)
    t_p0.arrived()
    d_n.start(0)
    outs.pass_on(-1)
    outs.pass_on(1)

    @pl.when(y == SIDE - 1)
    def _():
        c_x.arrived()
        cols_row[...] = summed(cols_chip[...], cols_x)
        c_z.start()

    ins.finish()

    def spread(kv, rows, at):
        first = lax.broadcasted_iota(jnp.int32, (rows, 128), 1) < HEAD_DIM
        turned = pltpu.roll(kv, HEAD_DIM, 1)
        kp0[at, :] = jnp.where(first, kv, 0.0).astype(BF16)
        kp1[at, :] = jnp.where(first, 0.0, turned).astype(BF16)
        vp0[at, :] = jnp.where(first, turned, 0.0).astype(BF16)
        vp1[at, :] = jnp.where(first, 0.0, kv).astype(BF16)

    last = pl.ds(ROWS, WINDOW)
    after = (lax.rem(sp + 1, PLANE), tp)
    halo = groups.new(pext.at[pl.ds(0, 2 * WINDOW)])
    halo.add(kvsend, kvland, after)
    halo.add(pext.at[last], pext.at[pl.ds(0, WINDOW)], after)

    def project(yy):
        at = rows_of(yy * CHUNK, CHUNK)
        got = jnp.dot(tok[at, :], win[...], preferred_element_type=F32)
        qbuf[at, :] = got[:, :128].astype(BF16)
        ahead = rows_of(yy * CHUNK + WINDOW, CHUNK)
        spread(got[:, 128:256].astype(BF16).astype(F32), CHUNK, ahead)
        pool = got[:, 256:].astype(BF16)
        pext[ahead, :] = pool
        sums = jnp.sum(pool.astype(F32).reshape(2, BLOCK // 8, 8, 128), axis=1)
        totals[pl.ds(yy * 2, 2)] = sums

        @pl.when(yy == SIDE - 1)
        def _():
            kvsend[...] = kp0[last, :] + vp1[last, :]
            halo.start()

    f_n.arrived()
    d_f.start(0)
    f_p.arrived()
    d_f.start(1)
    d_own.arrived()
    d_p.arrived()
    d_n.arrived()
    project(jnp.where(y == 0, yp, jnp.where(y == 3, y, yn)))
    project(jnp.where(y == 3, yp, y))
    project(jnp.where((y == 0) | (y == 3), yn, yp))
    outs.pass_on(2)

    @pl.when(y == SIDE - 1)
    def _():
        c_z.arrived()
        nothing = jnp.zeros((1, D), F32)
        ahead = summed(nothing, cols_z, z) + summed(nothing, cols_x, x)
        high = ahead.astype(BF16).astype(F32)
        middle = (ahead - high).astype(BF16).astype(F32)
        low = ahead - high - middle
        term = lax.broadcasted_iota(jnp.int32, (16, D), 0)
        rest = jnp.where(term == 1, middle, jnp.where(term == 2, low, 0.0))
        terms[...] = jnp.where(term == 0, high, rest).astype(BF16)

    d_f.arrived()
    project(yf)
    outs.finish()

    @pl.when(y == SIDE - 1)
    def _():
        got = jnp.dot(terms[...], win[:, 256:], preferred_element_type=F32)
        before[...] = jnp.sum(got, axis=0, keepdims=True)

    span = WINDOW + BLOCK
    q_index = lax.broadcasted_iota(jnp.int32, (BLOCK, span), 0)
    k_index = lax.broadcasted_iota(jnp.int32, (BLOCK, span), 1)
    distance = q_index + WINDOW - k_index
    reach = jnp.where(y == 0, 8, jnp.where(y == 1, 32, jnp.where(y == 2, WINDOW, 1 << 24)))
    inside = (distance >= 0) & (distance < WINDOW)
    banded = (distance >= 0) & (distance < reach) & ((k_index >= WINDOW) | (y < 3))
    sinks = (sink[:, 0:1], sink[:, 1:2])
    pool_gain = pgain[...]

    def probabilities(q, keys, allowed, sink):
        scores = lax.dot_general(q, keys, (((1,), (1,)), ((), ())), preferred_element_type=F32)
        scores = jnp.where(allowed, scores * HEAD_DIM ** (-0.5), -jnp.inf)
        peak = jnp.maximum(jnp.max(scores, axis=1, keepdims=True), sink)
        expo = jnp.exp(scores - peak)
        denom = jnp.sum(expo, axis=1, keepdims=True) + jnp.exp(sink - peak)
        return (expo * (1.0 / denom)).astype(BF16)

    def attend(yy, cc):
        number = yy * 2 + cc
        start = sp * ROWS + number * BLOCK
        at, pair = rows_of(number * BLOCK, BLOCK), rows_of(number * BLOCK, span)
        present = k_index >= WINDOW - start
        allowed, band = inside & present, banded & present
        q = qbuf[at, :]
        p0 = probabilities(q, kp0[pair, :], allowed, sinks[0])
        p1 = probabilities(q, kp1[pair, :], allowed, sinks[1])
        mixed = jnp.dot(p0, vp0[pair, :], preferred_element_type=F32)
        mixed = mixed + jnp.dot(p1, vp1[pair, :], preferred_element_type=F32)
        amine[at, pl.ds(0, 128)] = mixed.astype(BF16)
        ones = jnp.where(band, 1.0, 0.0).astype(BF16)
        sums = jnp.dot(ones, pext[pair, :], preferred_element_type=F32)
        earlier = lax.broadcasted_iota(jnp.int32, (2 * SIDE, 8, 128), 0) < number
        carry = jnp.sum(jnp.sum(jnp.where(earlier, totals[...], 0.0), axis=0), axis=0, keepdims=True)
        carry = jnp.where(y == 3, carry + before[...], 0.0)
        position = start + lax.broadcasted_iota(jnp.int32, (BLOCK, 128), 0)
        count = jnp.minimum(position + 1, reach).astype(F32)
        value = pext[rows_of(number * BLOCK + WINDOW, BLOCK), :].astype(F32)
        pooled = (sums + carry) / count
        amine[at, pl.ds(128, 128)] = ((pooled - value) * pool_gain).astype(BF16)

    def first_half(yy):
        @pl.when(yy == 0)
        def _():
            halo.arrived()
            spread(kvland[...].astype(F32), WINDOW, pl.ds(0, WINDOW))

        attend(yy, other)
        src = amine.at[rows_of((yy * 2 + other) * BLOCK, BLOCK)]
        dst = apart.at[rows_of(yy * BLOCK, BLOCK)]
        swap = one(src, dst, partner, dst)
        swap.start()
        return swap

    def product(yy, slot):
        mine = amine[rows_of((yy * 2 + c) * BLOCK, BLOCK), :]
        theirs = apart[rows_of(yy * BLOCK, BLOCK), :]
        for n in range(0, D, 512):
            cols = pl.ds(n, 512)
            got = jnp.dot(mine, wout[pl.ds(0, 256), cols], preferred_element_type=F32)
            got = got + jnp.dot(theirs, wout[pl.ds(256, 256), cols], preferred_element_type=F32)
            exact[slot, :, cols] = got
            if slot < 3:
                rounded[slot, :, cols] = got.astype(BF16)

    late = y == 2
    order = [jnp.where(late, u, v) for u, v in ((yn, yf), (yp, yn), (yf, yp))]
    at_far, at_next, at_prev = [jnp.where(late, u, v) for u, v in ((2, 0), (0, 1), (1, 2))]
    lower = [pl.ds(n * PART, PART) for n in range(HALF // PART)]
    upper = [pl.ds(HALF + n * PART, PART) for n in range(HALF // PART)]
    r_fn = [one(rounded.at[at_far, p], from_prev.at[1, p], up, from_prev.at[1, p]) for p in lower]
    r_fp = [one(rounded.at[at_far, p], from_next.at[1, p], down, from_next.at[1, p]) for p in upper]
    r_n1 = groups.new(from_prev.at[0, pl.ds(HALF, HALF)])
    r_p0 = groups.new(from_next.at[0, pl.ds(0, HALF)])
    for p, q in zip(lower, upper):
        r_n1.add(rounded.at[at_next, q], from_prev.at[0, q], up)
        r_p0.add(rounded.at[at_prev, p], from_next.at[0, p], down)
    r_n0 = [one(rounded.at[at_next, p], from_prev.at[0, p], up, from_prev.at[0, p]) for p in lower]
    r_p1 = [one(rounded.at[at_prev, p], from_next.at[0, p], down, from_next.at[0, p]) for p in upper]
    parts = range(len(lower))

    def send_far():
        for n in parts:
            r_fn[n].start()
            r_fp[n].start()

    swap_a = first_half(order[0])
    attend(order[0], c)
    swap_b = first_half(order[1])
    outs.shares.arrived()
    swap_a.arrived()
    product(order[0], 0)

    @pl.when(late)
    def _():
        r_n1.start(*parts[:EARLY])

    @pl.when(y != 2)
    def _():
        send_far()

    attend(order[1], c)
    swap_b.arrived()
    product(order[1], 1)

    @pl.when(late)
    def _():
        r_p0.start(*parts[:EARLY])

    @pl.when(y != 2)
    def _():
        r_n1.start()

    swap_c = first_half(order[2])
    attend(order[2], c)
    swap_d = first_half(y)
    swap_c.arrived()
    product(order[2], 2)

    @pl.when(late)
    def _():
        send_far()
        if EARLY < len(parts):
            r_n1.start(*parts[EARLY:])
            r_p0.start(*parts[EARLY:])

    @pl.when(y != 2)
    def _():
        r_p0.start()

    attend(y, c)
    for n in parts:
        r_fn[n].arrived()
        rounded[at_next, lower[n], :] = (
            exact[at_next, lower[n], :] + from_prev[1, lower[n], :].astype(F32)
        ).astype(BF16)
        r_n0[n].start()
        r_fp[n].arrived()
        rounded[at_prev, upper[n], :] = (
            exact[at_prev, upper[n], :] + from_next[1, upper[n], :].astype(F32)
        ).astype(BF16)
        r_p1[n].start()

    swap_d.arrived()
    product(y, 3)
    r_n1.arrived()
    for p in upper:
        exact[3, p, :] = exact[3, p, :] + from_prev[0, p, :].astype(F32)
    r_p0.arrived()
    for p in lower:
        exact[3, p, :] = exact[3, p, :] + from_next[0, p, :].astype(F32)
    for n in parts:
        for group, p, got in ((r_n0[n], lower[n], from_prev), (r_p1[n], upper[n], from_next)):
            group.arrived()
            result[p, :] = (exact[3, p, :] + got[0, p, :].astype(F32)).astype(BF16)
            pltpu.make_async_copy(result.at[p], out_hbm.at[p], out_sems.at[0]).start()
    pltpu.make_async_copy(result, out_hbm, out_sems.at[0]).wait()
    for group in groups.made:
        if group not in prefix_groups:
            group.sent()

    @pl.when(y == SIDE - 1)
    def _():
        for group in prefix_groups:
            group.sent()

    assert len(groups.made) == N_GROUPS, len(groups.made)


def local(
    tokens_in,
    norm_gain,
    query_weight,
    key_weight,
    value_weight,
    pool_weight,
    sink_logit,
    pool_gain,
    attention_out_weight,
    pool_out_weight,
):
    hbm = pl.BlockSpec(memory_space=pltpu.HBM)
    scratch = [
        ((BLOCK, D), BF16),
        ((1, D), F32),
        ((1, 128), F32),
        ((1, 2), F32),
        ((DEPTH, DEPTH), BF16),
        ((ROWS, D), BF16),
        ((D, IN_COLS), BF16),
        ((512, D), BF16),
        ((ROWS, 128), BF16),
        ((WINDOW, 128), BF16),
        ((WINDOW, 128), BF16),
        ((ROWS + WINDOW, 128), BF16),
        ((ROWS + WINDOW, 128), BF16),
        ((ROWS + WINDOW, 128), BF16),
        ((ROWS + WINDOW, 128), BF16),
        ((ROWS + WINDOW, 128), BF16),
        ((2 * SIDE, 8, 128), F32),
        ((1, 128), F32),
        ((1, D), F32),
        ((3, 1, D), F32),
        ((1, D), F32),
        ((1, D), F32),
        ((1, D), F32),
        ((1, D), F32),
        ((3, 1, D), F32),
        ((3, 1, D), F32),
        ((16, D), BF16),
        ((ROWS, 256), BF16),
        ((SIDE * BLOCK, 256), BF16),
        ((4, BLOCK, D), F32),
        ((3, BLOCK, D), BF16),
        ((2, BLOCK, D), BF16),
        ((2, BLOCK, D), BF16),
        ((BLOCK, D), BF16),
    ]
    return pl.pallas_call(
        kernel,
        out_shape=jax.ShapeDtypeStruct((BLOCK, D), BF16),
        in_specs=[hbm] * 10,
        out_specs=pl.BlockSpec(memory_space=pl.ANY),
        scratch_shapes=[pltpu.VMEM(shape, kind) for shape, kind in scratch]
        + [
            pltpu.SemaphoreType.DMA((7,)),
            pltpu.SemaphoreType.DMA((1,)),
            pltpu.SemaphoreType.DMA((N_GROUPS,)),
            pltpu.SemaphoreType.DMA((N_GROUPS,)),
        ],
        compiler_params=pltpu.CompilerParams(
            collective_id=0, has_side_effects=True, vmem_limit_bytes=62 * 1024 * 1024
        ),
    )(
        tokens_in,
        norm_gain.reshape(1, D),
        query_weight,
        key_weight.T,
        value_weight.T,
        pool_weight,
        sink_logit.reshape(1, 2),
        pool_gain.reshape(1, 128),
        attention_out_weight,
        pool_out_weight,
    )


def solution(mesh):
    in_specs = (
        P(("sp", "tp"), None),
        P(),
        P("sp", "tp"),
        P("sp", "tp"),
        P("sp", "tp"),
        P("sp", "tp"),
        P("tp"),
        P("tp"),
        P("tp", "sp"),
        P("tp", "sp"),
    )
    out_specs = P(("sp", "tp"), None)
    return jax.shard_map(local, mesh=mesh, in_specs=in_specs, out_specs=out_specs, check_vma=False)
```

```python
import math

import jax
import jax.numpy as jnp
from jax import lax
from jax.experimental import pallas as pl
from jax.experimental.pallas import tpu as pltpu
from jax.sharding import PartitionSpec as P

MESH = pl.DeviceIdType.MESH
F32 = jnp.float32
BF16 = jnp.bfloat16

D = 2048
HEAD_DIM = 64
WINDOW = 128
EPS = 1e-06
SIDE = 4
PLANE = SIDE * SIDE
BLOCK = 96
HALF = BLOCK // 2
ROWS = 2 * SIDE * BLOCK
CHUNK = 2 * BLOCK
DEPTH = D // PLANE
IN_COLS = 384
N_GROUPS = 48
SEND_SEMS = 4
SENT_ROWS = 12800
PART = 16
EARLY = 2


class Groups:
    def __init__(self, send_sems, recv_sems):
        self.send_sems, self.recv_sems, self.made, self.lone = send_sems, recv_sems, [], []

    def new(self, whole, lone=False):
        number = len(self.made)
        place = SEND_SEMS + len(self.lone) if lone else number % SEND_SEMS
        group = Group(self.send_sems.at[place], self.recv_sems.at[number], whole)
        self.made.append(group)
        if lone:
            self.lone.append(group)
        return group

    def one(self, src, dst, device, land):
        group = self.new(land)
        group.add(src, dst, device)
        return group

    def all_sent(self, rows):
        for n in range(SEND_SEMS):
            here = [g for g in self.made[n::SEND_SEMS] if g not in self.lone]
            size = sum(math.prod(g.whole.shape) * g.whole.dtype.itemsize for g in here)
            assert size % 4096 == 0 and size <= SENT_ROWS * 256, size
            part = rows.at[pl.ds(0, size // 256)]
            here[0].copy(part, part, here[0].device).wait_send()


class Group:
    def __init__(self, send_sem, recv_sem, whole):
        self.send_sem, self.recv_sem, self.whole, self.copies = send_sem, recv_sem, whole, []

    def copy(self, src, dst, device):
        return pltpu.make_async_remote_copy(
            src_ref=src,
            dst_ref=dst,
            send_sem=self.send_sem,
            recv_sem=self.recv_sem,
            device_id=device,
            device_id_type=MESH,
        )

    def add(self, src, dst, device):
        self.device = device
        self.copies.append((src, dst, device))
        return len(self.copies) - 1

    def start(self, *which):
        for n in which or range(len(self.copies)):
            self.copy(*self.copies[n]).start()

    def arrived(self):
        self.copy(self.whole, self.whole, self.device).wait_recv()

    def sent(self):
        self.copy(self.whole, self.whole, self.device).wait_send()


def rows_of(start, size, unit=16):
    return pl.ds(pl.multiple_of(start, unit), size)


def kernel(
    x_hbm,
    gain_hbm,
    wq_hbm,
    wk_hbm,
    wv_hbm,
    wp_hbm,
    sink_hbm,
    pgain_hbm,
    wa_hbm,
    wo_hbm,
    own_hbm,
    last_hbm,
    xin,
    gain,
    pgain,
    sink,
    wkv,
    tok,
    win,
    wout,
    qbuf,
    kvsend,
    kvland,
    kp0,
    kp1,
    vp0,
    vp1,
    pext,
    totals,
    before,
    cols_own,
    cols_y,
    cols_core,
    cols_other,
    cols_chip,
    cols_row,
    cols_x,
    cols_z,
    terms,
    amine,
    apart,
    exact,
    rounded,
    far_prev,
    far_next,
    near,
    sent,
    local_sems,
    out_sems,
    send_sems,
    recv_sems,
):
    sp = lax.axis_index("sp")
    tp = lax.axis_index("tp")
    z, x = sp // SIDE, lax.rem(sp, SIDE)
    y, c = tp // 2, lax.rem(tp, 2)
    other = 1 - c

    def turn(i, by):
        return lax.rem(i + by + SIDE, SIDE)

    yn, yp, yf = turn(y, 1), turn(y, -1), turn(y, 2)
    partner = (sp, y * 2 + other)
    up, down = (sp, yn * 2 + c), (sp, yp * 2 + c)

    barrier = pltpu.get_barrier_semaphore()
    beside = [(z * SIDE + turn(x, by), tp) for by in (1, -1)]
    above = [(turn(z, by) * SIDE + x, tp) for by in (1, -1)]
    opposite = [(z * SIDE + turn(x, 2), tp), (turn(z, 2) * SIDE + x, tp), (sp, yf * 2 + c)]
    peers = [up, down, partner] + beside + above + opposite
    for peer in peers:
        pl.semaphore_signal(barrier, inc=1, device_id=peer, device_id_type=MESH)

    own_in = rows_of(sp * DEPTH, DEPTH, 128)
    own_cols = rows_of(sp * 128, 128, 128)
    loads = [
        (0, x_hbm, xin),
        (1, gain_hbm, gain),
        (2, wk_hbm, wkv.at[pl.ds(0, HEAD_DIM)]),
        (2, wv_hbm, wkv.at[pl.ds(HEAD_DIM, HEAD_DIM)]),
        (3, wq_hbm, win.at[own_in, pl.ds(0, 128)]),
        (3, wp_hbm, win.at[own_in, pl.ds(256, 128)]),
        (4, wa_hbm, wout.at[pl.ds(0, 128), own_cols]),
        (4, wo_hbm, wout.at[pl.ds(128, 128), own_cols]),
        (5, pgain_hbm, pgain),
        (6, sink_hbm, sink),
    ]
    for n, src, dst in loads:
        pltpu.make_async_copy(src, dst, local_sems.at[n]).start()

    def loaded(n, whole):
        pltpu.make_async_copy(whole, whole, local_sems.at[n]).wait()

    loaded(0, xin)
    loaded(1, gain)
    gains = gain[...]

    def column_sums(rows):
        return jnp.sum(rows.astype(F32), axis=0, keepdims=True)

    columns = jnp.zeros((1, D), F32)
    for r in range(0, BLOCK, 16):
        wide = xin[pl.ds(r, 16)].astype(F32)
        inverse = lax.rsqrt(jnp.mean(wide * wide, axis=1, keepdims=True) + EPS)
        normed = (wide * inverse * gains).astype(BF16)
        tok[rows_of(tp * BLOCK + r, 16), :] = normed
        columns = columns + column_sums(normed)
    cols_own[...] = columns
    loaded(2, wkv)
    win[own_in, pl.ds(128, 128)] = wkv[...].T
    loaded(3, win.at[own_in, pl.ds(0, 256)])
    loaded(4, wout.at[pl.ds(0, 256), own_cols])
    loaded(5, pgain)
    loaded(6, sink)

    groups = Groups(send_sems, recv_sems)

    def block(yy, cc):
        return tok.at[rows_of((yy * 2 + cc) * BLOCK, BLOCK)]

    def half(yy, cc, h):
        return tok.at[rows_of((yy * 2 + cc) * BLOCK + h * HALF, HALF)]

    one = groups.one
    c_y = groups.new(cols_y)
    for n, by in enumerate((1, -1, 2)):
        c_y.add(cols_own, cols_y.at[n], (sp, turn(y, by) * 2 + c))
    t_n0 = one(half(y, c, 0), half(y, c, 0), up, half(yp, c, 0))
    t_p1 = one(half(y, c, 1), half(y, c, 1), down, half(yn, c, 1))
    t_n1 = one(half(y, c, 1), half(y, c, 1), up, half(yp, c, 1))
    t_p0 = one(half(y, c, 0), half(y, c, 0), down, half(yn, c, 0))
    f_n = one(half(yp, c, 0), half(yp, c, 0), up, half(yf, c, 0))
    f_p = one(half(yn, c, 1), half(yn, c, 1), down, half(yf, c, 1))
    d_own = one(block(y, c), block(y, c), partner, block(y, other))

    def across(yy):
        group = groups.new(block(yy, other))
        for h in range(2):
            group.add(half(yy, c, h), half(yy, c, h), partner)
        return group

    d_p, d_n, d_f = across(yp), across(yn), across(yf)
    c_core = one(cols_core, cols_other, partner, cols_other)
    c_x, c_z = groups.new(cols_x, True), groups.new(cols_z, True)
    for n, by in enumerate((1, -1, 2)):
        c_x.add(cols_chip, cols_x.at[n], (z * SIDE + turn(x, by), tp))
        c_z.add(cols_row, cols_z.at[n], (turn(z, by) * SIDE + x, tp))

    def summed(own, slots, here=None):
        total = own
        for n, by in enumerate((-1, 1, 2)):
            if here is None:
                total = total + slots[n]
            else:
                total = total + jnp.where(turn(here, by) < here, slots[n], 0.0)
        return total

    class Gather:
        def __init__(self, piece, sub, whole, direct, crossing_direct, shared=None):
            def source(g, o1, o2):
                if g == 0:
                    return turn(z, o2) * SIDE + turn(x, o1)
                return turn(z, o1) * SIDE + turn(x, o2)

            def put(group, ref, g, o1, o2):
                return group.add(ref, ref, (source(g, o1, o2), tp))

            self.first = groups.new(whole(4))
            self.first_far = groups.new(whole(2))
            self.last = groups.new(whole(8))
            self.direct = direct
            self.second, self.forward = {}, {}
            for g in range(2):
                mine = piece(g, source(g, 0, 0))
                put(self.first, mine, g, 1, 0)
                put(self.first, mine, g, -1, 0)
                if direct:
                    put(self.first_far, mine, g, 2, 0)
                else:
                    put(self.first_far, sub(g, source(g, -1, 0), 0), g, 1, 0)
                    put(self.first_far, sub(g, source(g, 1, 0), 1), g, -1, 0)
            for o in (0, -1, 1, 2):
                self.second[o] = groups.new(whole(4))
                self.forward[o] = []
                for g in range(2):
                    have = piece(g, source(g, o, 0))
                    put(self.second[o], have, g, 0, 1)
                    put(self.second[o], have, g, 0, -1)
                    if o in crossing_direct:
                        self.forward[o].append(put(self.last, have, g, 0, 2))
                    else:
                        low, high = sub(g, source(g, o, -1), 0), sub(g, source(g, o, 1), 1)
                        self.forward[o].append(put(self.last, low, g, 0, 1))
                        self.forward[o].append(put(self.last, high, g, 0, -1))
            self.crossing_direct = crossing_direct
            self.shares = None
            if shared:
                self.shares = groups.new(shared[0])
                self.share_of = {}
                for o1 in (0, -1, 1, 2):
                    for o2 in (0, -1, 1, 2):
                        self.share_of[o1, o2] = [
                            self.shares.add(
                                piece(g, source(g, o1, o2)), shared[1](g, source(g, o1, o2)), partner
                            )
                            for g in range(2)
                        ]

        def share(self, o1, o2):
            if self.shares:
                self.shares.start(*self.share_of[o1, o2])

        def begin(self):
            self.first.start()
            if self.direct:
                self.first_far.start()

        def cross(self, o):
            self.second[o].start()
            if o in self.crossing_direct:
                self.last.start(*self.forward[o])
            self.share(o, 0)

        def near(self):
            self.first.arrived()
            if not self.direct:
                self.first_far.start()
            self.cross(-1)
            self.cross(1)

        def distant(self):
            self.first_far.arrived()
            self.cross(2)

        def pass_on(self, o):
            self.second[o].arrived()
            if o not in self.crossing_direct:
                self.last.start(*self.forward[o])
            self.share(o, -1)
            self.share(o, 1)

        def finish(self):
            self.last.arrived()
            for o in (0, -1, 1, 2):
                self.share(o, 2)

    size = DEPTH // 2
    ins = Gather(
        lambda g, s: win.at[rows_of(s * DEPTH + g * size, size)],
        lambda g, s, h: win.at[rows_of(s * DEPTH + g * size + h * (size // 2), size // 2)],
        lambda n: win.at[pl.ds(0, n * size)],
        True,
        (),
    )
    outs = Gather(
        lambda g, s: wout.at[pl.ds(g * 128, 128), rows_of(s * 128, 128, 128)],
        lambda g, s, h: wout.at[pl.ds(g * 128 + h * 64, 64), rows_of(s * 128, 128, 128)],
        lambda n: wout.at[pl.ds(0, n * 8)],
        False,
        (2,),
        (
            wout.at[pl.ds(256, 256)],
            lambda g, s: wout.at[pl.ds(256 + g * 128, 128), rows_of(s * 128, 128, 128)],
        ),
    )

    pl.semaphore_wait(barrier, len(peers))

    for group in (c_y, t_n0, t_p1, t_n1, t_p0):
        group.start()
    ins.begin()
    ins.cross(0)
    outs.begin()
    outs.cross(0)
    d_own.start()
    ins.near()
    ins.distant()
    c_y.arrived()
    own_parity = summed(columns, cols_y)
    cols_core[...] = own_parity
    c_core.start()
    outs.near()
    ins.pass_on(0)
    c_core.arrived()
    cols_chip[...] = own_parity + cols_other[...]

    @pl.when(y == SIDE - 1)
    def _():
        c_x.start()

    t_n0.arrived()
    f_n.start()
    d_p.start(0)
    t_p1.arrived()
    f_p.start()
    d_n.start(1)
    outs.pass_on(0)
    ins.pass_on(-1)
    ins.pass_on(1)
    ins.pass_on(2)
    outs.distant()

    t_n1.arrived()
    d_p.start(1)
    t_p0.arrived()
    d_n.start(0)
    outs.pass_on(-1)
    outs.pass_on(1)

    @pl.when(y == SIDE - 1)
    def _():
        c_x.arrived()
        cols_row[...] = summed(cols_chip[...], cols_x)
        c_z.start()

    ins.finish()

    def spread(kv, rows, at):
        first = lax.broadcasted_iota(jnp.int32, (rows, 128), 1) < HEAD_DIM
        turned = pltpu.roll(kv, HEAD_DIM, 1)
        kp0[at, :] = jnp.where(first, kv, 0.0).astype(BF16)
        kp1[at, :] = jnp.where(first, 0.0, turned).astype(BF16)
        vp0[at, :] = jnp.where(first, turned, 0.0).astype(BF16)
        vp1[at, :] = jnp.where(first, 0.0, kv).astype(BF16)

    last = pl.ds(ROWS, WINDOW)
    after = (lax.rem(sp + 1, PLANE), tp)
    halo = groups.new(pext.at[pl.ds(0, 2 * WINDOW)])
    halo.add(kvsend, kvland, after)
    halo.add(pext.at[last], pext.at[pl.ds(0, WINDOW)], after)

    def project(yy):
        at = rows_of(yy * CHUNK, CHUNK)
        got = jnp.dot(tok[at, :], win[...], preferred_element_type=F32)
        qbuf[at, :] = got[:, :128].astype(BF16)
        ahead = rows_of(yy * CHUNK + WINDOW, CHUNK)
        spread(got[:, 128:256].astype(BF16).astype(F32), CHUNK, ahead)
        pool = got[:, 256:].astype(BF16)
        pext[ahead, :] = pool
        sums = jnp.sum(pool.astype(F32).reshape(2, BLOCK // 8, 8, 128), axis=1)
        totals[pl.ds(yy * 2, 2)] = sums

        @pl.when(yy == SIDE - 1)
        def _():
            kvsend[...] = kp0[last, :] + vp1[last, :]
            halo.start()

    f_n.arrived()
    d_f.start(0)
    f_p.arrived()
    d_f.start(1)
    d_own.arrived()
    d_p.arrived()
    d_n.arrived()
    project(jnp.where(y == 0, yp, jnp.where(y == 3, y, yn)))
    project(jnp.where(y == 3, yp, y))
    project(jnp.where((y == 0) | (y == 3), yn, yp))
    outs.pass_on(2)

    @pl.when(y == SIDE - 1)
    def _():
        c_z.arrived()
        nothing = jnp.zeros((1, D), F32)
        ahead = summed(nothing, cols_z, z) + summed(nothing, cols_x, x)
        high = ahead.astype(BF16).astype(F32)
        middle = (ahead - high).astype(BF16).astype(F32)
        low = ahead - high - middle
        term = lax.broadcasted_iota(jnp.int32, (16, D), 0)
        rest = jnp.where(term == 1, middle, jnp.where(term == 2, low, 0.0))
        terms[...] = jnp.where(term == 0, high, rest).astype(BF16)

    d_f.arrived()
    project(yf)
    outs.finish()

    @pl.when(y == SIDE - 1)
    def _():
        got = jnp.dot(terms[...], win[:, 256:], preferred_element_type=F32)
        before[...] = jnp.sum(got, axis=0, keepdims=True)

    span = WINDOW + BLOCK
    q_index = lax.broadcasted_iota(jnp.int32, (BLOCK, span), 0)
    k_index = lax.broadcasted_iota(jnp.int32, (BLOCK, span), 1)
    distance = q_index + WINDOW - k_index
    reach = jnp.where(y == 0, 8, jnp.where(y == 1, 32, jnp.where(y == 2, WINDOW, 1 << 24)))
    inside = (distance >= 0) & (distance < WINDOW)
    banded = (distance >= 0) & (distance < reach) & ((k_index >= WINDOW) | (y < 3))
    sinks = (sink[:, 0:1], sink[:, 1:2])
    pool_gain = pgain[...]

    def probabilities(q, keys, allowed, sink):
        scores = lax.dot_general(q, keys, (((1,), (1,)), ((), ())), preferred_element_type=F32)
        scores = jnp.where(allowed, scores * HEAD_DIM ** (-0.5), -jnp.inf)
        peak = jnp.maximum(jnp.max(scores, axis=1, keepdims=True), sink)
        expo = jnp.exp(scores - peak)
        denom = jnp.sum(expo, axis=1, keepdims=True) + jnp.exp(sink - peak)
        return (expo * (1.0 / denom)).astype(BF16)

    def attend(yy, cc):
        number = yy * 2 + cc
        start = sp * ROWS + number * BLOCK
        at, pair = rows_of(number * BLOCK, BLOCK), rows_of(number * BLOCK, span)
        present = k_index >= WINDOW - start
        allowed, band = inside & present, banded & present
        q = qbuf[at, :]
        p0 = probabilities(q, kp0[pair, :], allowed, sinks[0])
        p1 = probabilities(q, kp1[pair, :], allowed, sinks[1])
        mixed = jnp.dot(p0, vp0[pair, :], preferred_element_type=F32)
        mixed = mixed + jnp.dot(p1, vp1[pair, :], preferred_element_type=F32)
        amine[at, pl.ds(0, 128)] = mixed.astype(BF16)
        ones = jnp.where(band, 1.0, 0.0).astype(BF16)
        sums = jnp.dot(ones, pext[pair, :], preferred_element_type=F32)
        earlier = lax.broadcasted_iota(jnp.int32, (2 * SIDE, 8, 128), 0) < number
        carry = jnp.sum(jnp.sum(jnp.where(earlier, totals[...], 0.0), axis=0), axis=0, keepdims=True)
        carry = jnp.where(y == 3, carry + before[...], 0.0)
        position = start + lax.broadcasted_iota(jnp.int32, (BLOCK, 128), 0)
        count = jnp.minimum(position + 1, reach).astype(F32)
        value = pext[rows_of(number * BLOCK + WINDOW, BLOCK), :].astype(F32)
        pooled = (sums + carry) / count
        amine[at, pl.ds(128, 128)] = ((pooled - value) * pool_gain).astype(BF16)

    def first_half(yy):
        @pl.when(yy == 0)
        def _():
            halo.arrived()
            spread(kvland[...].astype(F32), WINDOW, pl.ds(0, WINDOW))

        attend(yy, other)
        src = amine.at[rows_of((yy * 2 + other) * BLOCK, BLOCK)]
        dst = apart.at[rows_of(yy * BLOCK, BLOCK)]
        swap = one(src, dst, partner, dst)
        swap.start()
        return swap

    def product(yy, slot):
        mine = amine[rows_of((yy * 2 + c) * BLOCK, BLOCK), :]
        theirs = apart[rows_of(yy * BLOCK, BLOCK), :]
        for n in range(0, D, 512):
            cols = pl.ds(n, 512)
            got = jnp.dot(mine, wout[pl.ds(0, 256), cols], preferred_element_type=F32)
            got = got + jnp.dot(theirs, wout[pl.ds(256, 256), cols], preferred_element_type=F32)
            exact[slot, :, cols] = got
            if slot < 3:
                rounded[slot, :, cols] = got.astype(BF16)

    late = y == 2
    order = [jnp.where(late, u, v) for u, v in ((yn, yf), (yp, yn), (yf, yp))]
    at_far, at_next, at_prev = [jnp.where(late, u, v) for u, v in ((2, 0), (0, 1), (1, 2))]
    lower = [pl.ds(n * PART, PART) for n in range(HALF // PART)]
    upper = [pl.ds(HALF + n * PART, PART) for n in range(HALF // PART)]
    r_fn = [one(rounded.at[at_far, p], far_prev.at[p], up, far_prev.at[p]) for p in lower]
    r_fp = [one(rounded.at[at_far, p], far_next.at[p], down, far_next.at[p]) for p in upper]
    r_n1 = groups.new(near.at[pl.ds(HALF, HALF)])
    r_p0 = groups.new(near.at[pl.ds(0, HALF)])
    for p, q in zip(lower, upper):
        r_n1.add(rounded.at[at_next, q], near.at[q], up)
        r_p0.add(rounded.at[at_prev, p], near.at[p], down)
    r_n0 = [one(rounded.at[at_next, p], last_hbm.at[p], up, last_hbm.at[p]) for p in lower]
    r_p1 = [one(rounded.at[at_prev, p], last_hbm.at[p], down, last_hbm.at[p]) for p in upper]
    parts = range(len(lower))

    def send_far():
        for n in parts:
            r_fn[n].start()
            r_fp[n].start()

    swap_a = first_half(order[0])
    attend(order[0], c)
    swap_b = first_half(order[1])
    outs.shares.arrived()
    swap_a.arrived()
    product(order[0], 0)

    @pl.when(late)
    def _():
        r_n1.start(*parts[:EARLY])

    @pl.when(y != 2)
    def _():
        send_far()

    attend(order[1], c)
    swap_b.arrived()
    product(order[1], 1)

    @pl.when(late)
    def _():
        r_p0.start(*parts[:EARLY])

    @pl.when(y != 2)
    def _():
        r_n1.start()

    swap_c = first_half(order[2])
    attend(order[2], c)
    swap_d = first_half(y)
    swap_c.arrived()
    product(order[2], 2)

    @pl.when(late)
    def _():
        send_far()
        if EARLY < len(parts):
            r_n1.start(*parts[EARLY:])
            r_p0.start(*parts[EARLY:])

    @pl.when(y != 2)
    def _():
        r_p0.start()

    attend(y, c)
    for n in parts:
        r_fn[n].arrived()
        rounded[at_next, lower[n], :] = (
            exact[at_next, lower[n], :] + far_prev[lower[n], :].astype(F32)
        ).astype(BF16)
        r_n0[n].start()
        r_fp[n].arrived()
        rounded[at_prev, upper[n], :] = (
            exact[at_prev, upper[n], :] + far_next[upper[n], :].astype(F32)
        ).astype(BF16)
        r_p1[n].start()

    swap_d.arrived()
    product(y, 3)
    r_n1.arrived()
    r_p0.arrived()
    for p in lower + upper:
        exact[3, p, :] = exact[3, p, :] + near[p, :].astype(F32)
    mine = pltpu.make_async_copy(exact.at[3], own_hbm, out_sems.at[0])
    mine.start()
    for n in parts:
        r_n0[n].arrived()
        r_p1[n].arrived()
    mine.wait()
    groups.all_sent(sent)

    @pl.when(y == SIDE - 1)
    def _():
        c_x.sent()
        c_z.sent()

    assert len(groups.made) == N_GROUPS, len(groups.made)


def local(
    tokens_in,
    norm_gain,
    query_weight,
    key_weight,
    value_weight,
    pool_weight,
    sink_logit,
    pool_gain,
    attention_out_weight,
    pool_out_weight,
):
    hbm = pl.BlockSpec(memory_space=pltpu.HBM)
    scratch = [
        ((BLOCK, D), BF16),
        ((1, D), F32),
        ((1, 128), F32),
        ((1, 2), F32),
        ((DEPTH, DEPTH), BF16),
        ((ROWS, D), BF16),
        ((D, IN_COLS), BF16),
        ((512, D), BF16),
        ((ROWS, 128), BF16),
        ((WINDOW, 128), BF16),
        ((WINDOW, 128), BF16),
        ((ROWS + WINDOW, 128), BF16),
        ((ROWS + WINDOW, 128), BF16),
        ((ROWS + WINDOW, 128), BF16),
        ((ROWS + WINDOW, 128), BF16),
        ((ROWS + WINDOW, 128), BF16),
        ((2 * SIDE, 8, 128), F32),
        ((1, 128), F32),
        ((1, D), F32),
        ((3, 1, D), F32),
        ((1, D), F32),
        ((1, D), F32),
        ((1, D), F32),
        ((1, D), F32),
        ((3, 1, D), F32),
        ((3, 1, D), F32),
        ((16, D), BF16),
        ((ROWS, 256), BF16),
        ((SIDE * BLOCK, 256), BF16),
        ((4, BLOCK, D), F32),
        ((3, BLOCK, D), BF16),
        ((BLOCK, D), BF16),
        ((BLOCK, D), BF16),
        ((BLOCK, D), BF16),
        ((SENT_ROWS, 128), BF16),
    ]
    own, last = pl.pallas_call(
        kernel,
        out_shape=[
            jax.ShapeDtypeStruct((BLOCK, D), F32),
            jax.ShapeDtypeStruct((BLOCK, D), BF16),
        ],
        in_specs=[hbm] * 10,
        out_specs=[pl.BlockSpec(memory_space=pl.ANY)] * 2,
        scratch_shapes=[pltpu.VMEM(shape, kind) for shape, kind in scratch]
        + [
            pltpu.SemaphoreType.DMA((7,)),
            pltpu.SemaphoreType.DMA((1,)),
            pltpu.SemaphoreType.DMA((SEND_SEMS + 2,)),
            pltpu.SemaphoreType.DMA((N_GROUPS,)),
        ],
        compiler_params=pltpu.CompilerParams(
            collective_id=0, has_side_effects=True, vmem_limit_bytes=62 * 1024 * 1024
        ),
    )(
        tokens_in,
        norm_gain.reshape(1, D),
        query_weight,
        key_weight.T,
        value_weight.T,
        pool_weight,
        sink_logit.reshape(1, 2),
        pool_gain.reshape(1, 128),
        attention_out_weight,
        pool_out_weight,
    )
    return (own + last.astype(F32)).astype(BF16)


def solution(mesh):
    in_specs = (
        P(("sp", "tp"), None),
        P(),
        P("sp", "tp"),
        P("sp", "tp"),
        P("sp", "tp"),
        P("sp", "tp"),
        P("tp"),
        P("tp"),
        P("tp", "sp"),
        P("tp", "sp"),
    )
    out_specs = P(("sp", "tp"), None)
    return jax.shard_map(local, mesh=mesh, in_specs=in_specs, out_specs=out_specs, check_vma=False)
```

```python
import math

import jax
import jax.numpy as jnp
from jax import lax
from jax.experimental import pallas as pl
from jax.experimental.pallas import tpu as pltpu
from jax.sharding import PartitionSpec as P

MESH = pl.DeviceIdType.MESH
F32 = jnp.float32
BF16 = jnp.bfloat16

D = 2048
HEAD_DIM = 64
WINDOW = 128
EPS = 1e-06
SIDE = 4
PLANE = SIDE * SIDE
BLOCK = 96
HALF = BLOCK // 2
ROWS = 2 * SIDE * BLOCK
CHUNK = 2 * BLOCK
DEPTH = D // PLANE
IN_COLS = 384
N_GROUPS = 48
SEND_SEMS = 4
SENT_ROWS = 12800
PART = 16
EARLY = 2


class Groups:
    def __init__(self, send_sems, recv_sems):
        self.send_sems, self.recv_sems, self.made, self.lone = send_sems, recv_sems, [], []

    def new(self, whole, lone=False):
        number = len(self.made)
        place = SEND_SEMS + len(self.lone) if lone else number % SEND_SEMS
        group = Group(self.send_sems.at[place], self.recv_sems.at[number], whole)
        self.made.append(group)
        if lone:
            self.lone.append(group)
        return group

    def one(self, src, dst, device, land):
        group = self.new(land)
        group.add(src, dst, device)
        return group

    def all_sent(self, rows):
        for n in range(SEND_SEMS):
            here = [g for g in self.made[n::SEND_SEMS] if g not in self.lone]
            size = sum(math.prod(g.whole.shape) * g.whole.dtype.itemsize for g in here)
            assert size % 4096 == 0 and size <= SENT_ROWS * 256, size
            part = rows.at[pl.ds(0, size // 256)]
            here[0].copy(part, part, here[0].device).wait_send()


class Group:
    def __init__(self, send_sem, recv_sem, whole):
        self.send_sem, self.recv_sem, self.whole, self.copies = send_sem, recv_sem, whole, []

    def copy(self, src, dst, device):
        return pltpu.make_async_remote_copy(
            src_ref=src,
            dst_ref=dst,
            send_sem=self.send_sem,
            recv_sem=self.recv_sem,
            device_id=device,
            device_id_type=MESH,
        )

    def add(self, src, dst, device):
        self.device = device
        self.copies.append((src, dst, device))
        return len(self.copies) - 1

    def start(self, *which):
        for n in which or range(len(self.copies)):
            self.copy(*self.copies[n]).start()

    def arrived(self):
        self.copy(self.whole, self.whole, self.device).wait_recv()

    def sent(self):
        self.copy(self.whole, self.whole, self.device).wait_send()


def rows_of(start, size, unit=16):
    return pl.ds(pl.multiple_of(start, unit), size)


def kernel(
    x_hbm,
    gain_hbm,
    wq_hbm,
    wk_hbm,
    wv_hbm,
    wp_hbm,
    sink_hbm,
    pgain_hbm,
    wa_hbm,
    wo_hbm,
    own_hbm,
    last_hbm,
    xin,
    gain,
    pgain,
    sink,
    wkv,
    tok,
    win,
    wout,
    qbuf,
    kvsend,
    kvland,
    kp0,
    kp1,
    vp0,
    vp1,
    pext,
    totals,
    before,
    cols_own,
    cols_y,
    cols_core,
    cols_other,
    cols_chip,
    cols_row,
    cols_x,
    cols_z,
    terms,
    amine,
    apart,
    exact,
    rounded,
    far_prev,
    far_next,
    near,
    result,
    sent,
    local_sems,
    out_sems,
    send_sems,
    recv_sems,
):
    sp = lax.axis_index("sp")
    tp = lax.axis_index("tp")
    z, x = sp // SIDE, lax.rem(sp, SIDE)
    y, c = tp // 2, lax.rem(tp, 2)
    other = 1 - c

    def turn(i, by):
        return lax.rem(i + by + SIDE, SIDE)

    yn, yp, yf = turn(y, 1), turn(y, -1), turn(y, 2)
    partner = (sp, y * 2 + other)
    up, down = (sp, yn * 2 + c), (sp, yp * 2 + c)

    barrier = pltpu.get_barrier_semaphore()
    beside = [(z * SIDE + turn(x, by), tp) for by in (1, -1)]
    above = [(turn(z, by) * SIDE + x, tp) for by in (1, -1)]
    opposite = [(z * SIDE + turn(x, 2), tp), (turn(z, 2) * SIDE + x, tp), (sp, yf * 2 + c)]
    peers = [up, down, partner] + beside + above + opposite
    for peer in peers:
        pl.semaphore_signal(barrier, inc=1, device_id=peer, device_id_type=MESH)

    own_in = rows_of(sp * DEPTH, DEPTH, 128)
    own_cols = rows_of(sp * 128, 128, 128)
    loads = [
        (0, x_hbm, xin),
        (1, gain_hbm, gain),
        (2, wk_hbm, wkv.at[pl.ds(0, HEAD_DIM)]),
        (2, wv_hbm, wkv.at[pl.ds(HEAD_DIM, HEAD_DIM)]),
        (3, wq_hbm, win.at[own_in, pl.ds(0, 128)]),
        (3, wp_hbm, win.at[own_in, pl.ds(256, 128)]),
        (4, wa_hbm, wout.at[pl.ds(0, 128), own_cols]),
        (4, wo_hbm, wout.at[pl.ds(128, 128), own_cols]),
        (5, pgain_hbm, pgain),
        (6, sink_hbm, sink),
    ]
    for n, src, dst in loads:
        pltpu.make_async_copy(src, dst, local_sems.at[n]).start()

    def loaded(n, whole):
        pltpu.make_async_copy(whole, whole, local_sems.at[n]).wait()

    loaded(0, xin)
    loaded(1, gain)
    gains = gain[...]

    def column_sums(rows):
        return jnp.sum(rows.astype(F32), axis=0, keepdims=True)

    columns = jnp.zeros((1, D), F32)
    for r in range(0, BLOCK, 16):
        wide = xin[pl.ds(r, 16)].astype(F32)
        inverse = lax.rsqrt(jnp.mean(wide * wide, axis=1, keepdims=True) + EPS)
        normed = (wide * inverse * gains).astype(BF16)
        tok[rows_of(tp * BLOCK + r, 16), :] = normed
        columns = columns + column_sums(normed)
    cols_own[...] = columns
    loaded(2, wkv)
    win[own_in, pl.ds(128, 128)] = wkv[...].T
    loaded(3, win.at[own_in, pl.ds(0, 256)])
    loaded(4, wout.at[pl.ds(0, 256), own_cols])
    loaded(5, pgain)
    loaded(6, sink)

    groups = Groups(send_sems, recv_sems)

    def block(yy, cc):
        return tok.at[rows_of((yy * 2 + cc) * BLOCK, BLOCK)]

    def half(yy, cc, h):
        return tok.at[rows_of((yy * 2 + cc) * BLOCK + h * HALF, HALF)]

    one = groups.one
    c_y = groups.new(cols_y)
    for n, by in enumerate((1, -1, 2)):
        c_y.add(cols_own, cols_y.at[n], (sp, turn(y, by) * 2 + c))
    t_n0 = one(half(y, c, 0), half(y, c, 0), up, half(yp, c, 0))
    t_p1 = one(half(y, c, 1), half(y, c, 1), down, half(yn, c, 1))
    t_n1 = one(half(y, c, 1), half(y, c, 1), up, half(yp, c, 1))
    t_p0 = one(half(y, c, 0), half(y, c, 0), down, half(yn, c, 0))
    f_n = one(half(yp, c, 0), half(yp, c, 0), up, half(yf, c, 0))
    f_p = one(half(yn, c, 1), half(yn, c, 1), down, half(yf, c, 1))
    d_own = one(block(y, c), block(y, c), partner, block(y, other))

    def across(yy):
        group = groups.new(block(yy, other))
        for h in range(2):
            group.add(half(yy, c, h), half(yy, c, h), partner)
        return group

    d_p, d_n, d_f = across(yp), across(yn), across(yf)
    c_core = one(cols_core, cols_other, partner, cols_other)
    c_x, c_z = groups.new(cols_x, True), groups.new(cols_z, True)
    for n, by in enumerate((1, -1, 2)):
        c_x.add(cols_chip, cols_x.at[n], (z * SIDE + turn(x, by), tp))
        c_z.add(cols_row, cols_z.at[n], (turn(z, by) * SIDE + x, tp))

    def summed(own, slots, here=None):
        total = own
        for n, by in enumerate((-1, 1, 2)):
            if here is None:
                total = total + slots[n]
            else:
                total = total + jnp.where(turn(here, by) < here, slots[n], 0.0)
        return total

    class Gather:
        def __init__(self, piece, sub, whole, direct, crossing_direct, shared=None):
            def source(g, o1, o2):
                if g == 0:
                    return turn(z, o2) * SIDE + turn(x, o1)
                return turn(z, o1) * SIDE + turn(x, o2)

            def put(group, ref, g, o1, o2):
                return group.add(ref, ref, (source(g, o1, o2), tp))

            self.first = groups.new(whole(4))
            self.first_far = groups.new(whole(2))
            self.last = groups.new(whole(8))
            self.direct = direct
            self.second, self.forward = {}, {}
            for g in range(2):
                mine = piece(g, source(g, 0, 0))
                put(self.first, mine, g, 1, 0)
                put(self.first, mine, g, -1, 0)
                if direct:
                    put(self.first_far, mine, g, 2, 0)
                else:
                    put(self.first_far, sub(g, source(g, -1, 0), 0), g, 1, 0)
                    put(self.first_far, sub(g, source(g, 1, 0), 1), g, -1, 0)
            for o in (0, -1, 1, 2):
                self.second[o] = groups.new(whole(4))
                self.forward[o] = []
                for g in range(2):
                    have = piece(g, source(g, o, 0))
                    put(self.second[o], have, g, 0, 1)
                    put(self.second[o], have, g, 0, -1)
                    if o in crossing_direct:
                        self.forward[o].append(put(self.last, have, g, 0, 2))
                    else:
                        low, high = sub(g, source(g, o, -1), 0), sub(g, source(g, o, 1), 1)
                        self.forward[o].append(put(self.last, low, g, 0, 1))
                        self.forward[o].append(put(self.last, high, g, 0, -1))
            self.crossing_direct = crossing_direct
            self.shares = None
            if shared:
                self.shares = groups.new(shared[0])
                self.share_of = {}
                for o1 in (0, -1, 1, 2):
                    for o2 in (0, -1, 1, 2):
                        self.share_of[o1, o2] = [
                            self.shares.add(
                                piece(g, source(g, o1, o2)), shared[1](g, source(g, o1, o2)), partner
                            )
                            for g in range(2)
                        ]

        def share(self, o1, o2):
            if self.shares:
                self.shares.start(*self.share_of[o1, o2])

        def begin(self):
            self.first.start()
            if self.direct:
                self.first_far.start()

        def cross(self, o):
            self.second[o].start()
            if o in self.crossing_direct:
                self.last.start(*self.forward[o])
            self.share(o, 0)

        def near(self):
            self.first.arrived()
            if not self.direct:
                self.first_far.start()
            self.cross(-1)
            self.cross(1)

        def distant(self):
            self.first_far.arrived()
            self.cross(2)

        def pass_on(self, o):
            self.second[o].arrived()
            if o not in self.crossing_direct:
                self.last.start(*self.forward[o])
            self.share(o, -1)
            self.share(o, 1)

        def finish(self):
            self.last.arrived()
            for o in (0, -1, 1, 2):
                self.share(o, 2)

    size = DEPTH // 2
    ins = Gather(
        lambda g, s: win.at[rows_of(s * DEPTH + g * size, size)],
        lambda g, s, h: win.at[rows_of(s * DEPTH + g * size + h * (size // 2), size // 2)],
        lambda n: win.at[pl.ds(0, n * size)],
        True,
        (),
    )
    outs = Gather(
        lambda g, s: wout.at[pl.ds(g * 128, 128), rows_of(s * 128, 128, 128)],
        lambda g, s, h: wout.at[pl.ds(g * 128 + h * 64, 64), rows_of(s * 128, 128, 128)],
        lambda n: wout.at[pl.ds(0, n * 8)],
        False,
        (2,),
        (
            wout.at[pl.ds(256, 256)],
            lambda g, s: wout.at[pl.ds(256 + g * 128, 128), rows_of(s * 128, 128, 128)],
        ),
    )

    pl.semaphore_wait(barrier, len(peers))

    for group in (c_y, t_n0, t_p1, t_n1, t_p0):
        group.start()
    ins.begin()
    ins.cross(0)
    outs.begin()
    outs.cross(0)
    d_own.start()
    ins.near()
    ins.distant()
    c_y.arrived()
    own_parity = summed(columns, cols_y)
    cols_core[...] = own_parity
    c_core.start()
    outs.near()
    ins.pass_on(0)
    c_core.arrived()
    cols_chip[...] = own_parity + cols_other[...]

    @pl.when(y == SIDE - 1)
    def _():
        c_x.start()

    t_n0.arrived()
    f_n.start()
    d_p.start(0)
    t_p1.arrived()
    f_p.start()
    d_n.start(1)
    outs.pass_on(0)
    ins.pass_on(-1)
    ins.pass_on(1)
    ins.pass_on(2)
    outs.distant()

    t_n1.arrived()
    d_p.start(1)
    t_p0.arrived()
    d_n.start(0)
    outs.pass_on(-1)
    outs.pass_on(1)

    @pl.when(y == SIDE - 1)
    def _():
        c_x.arrived()
        cols_row[...] = summed(cols_chip[...], cols_x)
        c_z.start()

    ins.finish()

    def spread(kv, rows, at):
        first = lax.broadcasted_iota(jnp.int32, (rows, 128), 1) < HEAD_DIM
        turned = pltpu.roll(kv, HEAD_DIM, 1)
        kp0[at, :] = jnp.where(first, kv, 0.0).astype(BF16)
        kp1[at, :] = jnp.where(first, 0.0, turned).astype(BF16)
        vp0[at, :] = jnp.where(first, turned, 0.0).astype(BF16)
        vp1[at, :] = jnp.where(first, 0.0, kv).astype(BF16)

    last = pl.ds(ROWS, WINDOW)
    after = (lax.rem(sp + 1, PLANE), tp)
    halo = groups.new(pext.at[pl.ds(0, 2 * WINDOW)])
    halo.add(kvsend, kvland, after)
    halo.add(pext.at[last], pext.at[pl.ds(0, WINDOW)], after)

    def project(yy):
        at = rows_of(yy * CHUNK, CHUNK)
        got = jnp.dot(tok[at, :], win[...], preferred_element_type=F32)
        qbuf[at, :] = got[:, :128].astype(BF16)
        ahead = rows_of(yy * CHUNK + WINDOW, CHUNK)
        spread(got[:, 128:256].astype(BF16).astype(F32), CHUNK, ahead)
        pool = got[:, 256:].astype(BF16)
        pext[ahead, :] = pool
        sums = jnp.sum(pool.astype(F32).reshape(2, BLOCK // 8, 8, 128), axis=1)
        totals[pl.ds(yy * 2, 2)] = sums

        @pl.when(yy == SIDE - 1)
        def _():
            kvsend[...] = kp0[last, :] + vp1[last, :]
            halo.start()

    f_n.arrived()
    d_f.start(0)
    f_p.arrived()
    d_f.start(1)
    d_own.arrived()
    d_p.arrived()
    d_n.arrived()
    project(jnp.where(y == 0, yp, jnp.where(y == 3, y, yn)))
    project(jnp.where(y == 3, yp, y))
    project(jnp.where((y == 0) | (y == 3), yn, yp))

    @pl.when(y == SIDE - 1)
    def _():
        c_z.arrived()
        nothing = jnp.zeros((1, D), F32)
        ahead = summed(nothing, cols_z, z) + summed(nothing, cols_x, x)
        high = ahead.astype(BF16).astype(F32)
        middle = (ahead - high).astype(BF16).astype(F32)
        low = ahead - high - middle
        term = lax.broadcasted_iota(jnp.int32, (16, D), 0)
        rest = jnp.where(term == 1, middle, jnp.where(term == 2, low, 0.0))
        terms[...] = jnp.where(term == 0, high, rest).astype(BF16)

    d_f.arrived()
    project(yf)
    outs.pass_on(2)
    outs.finish()

    @pl.when(y == SIDE - 1)
    def _():
        got = jnp.dot(terms[...], win[:, 256:], preferred_element_type=F32)
        before[...] = jnp.sum(got, axis=0, keepdims=True)

    span = WINDOW + BLOCK
    q_index = lax.broadcasted_iota(jnp.int32, (BLOCK, span), 0)
    k_index = lax.broadcasted_iota(jnp.int32, (BLOCK, span), 1)
    distance = q_index + WINDOW - k_index
    reach = jnp.where(y == 0, 8, jnp.where(y == 1, 32, jnp.where(y == 2, WINDOW, 1 << 24)))
    inside = (distance >= 0) & (distance < WINDOW)
    banded = (distance >= 0) & (distance < reach) & ((k_index >= WINDOW) | (y < 3))
    sinks = (sink[:, 0:1], sink[:, 1:2])
    pool_gain = pgain[...]

    def probabilities(q, keys, allowed, sink):
        scores = lax.dot_general(q, keys, (((1,), (1,)), ((), ())), preferred_element_type=F32)
        scores = jnp.where(allowed, scores * HEAD_DIM ** (-0.5), -jnp.inf)
        peak = jnp.maximum(jnp.max(scores, axis=1, keepdims=True), sink)
        expo = jnp.exp(scores - peak)
        denom = jnp.sum(expo, axis=1, keepdims=True) + jnp.exp(sink - peak)
        return (expo * (1.0 / denom)).astype(BF16)

    def attend(yy, cc):
        number = yy * 2 + cc
        start = sp * ROWS + number * BLOCK
        at, pair = rows_of(number * BLOCK, BLOCK), rows_of(number * BLOCK, span)
        present = k_index >= WINDOW - start
        allowed, band = inside & present, banded & present
        q = qbuf[at, :]
        p0 = probabilities(q, kp0[pair, :], allowed, sinks[0])
        p1 = probabilities(q, kp1[pair, :], allowed, sinks[1])
        mixed = jnp.dot(p0, vp0[pair, :], preferred_element_type=F32)
        mixed = mixed + jnp.dot(p1, vp1[pair, :], preferred_element_type=F32)
        amine[at, pl.ds(0, 128)] = mixed.astype(BF16)
        ones = jnp.where(band, 1.0, 0.0).astype(BF16)
        sums = jnp.dot(ones, pext[pair, :], preferred_element_type=F32)
        earlier = lax.broadcasted_iota(jnp.int32, (2 * SIDE, 8, 128), 0) < number
        carry = jnp.sum(jnp.sum(jnp.where(earlier, totals[...], 0.0), axis=0), axis=0, keepdims=True)
        carry = jnp.where(y == 3, carry + before[...], 0.0)
        position = start + lax.broadcasted_iota(jnp.int32, (BLOCK, 128), 0)
        count = jnp.minimum(position + 1, reach).astype(F32)
        value = pext[rows_of(number * BLOCK + WINDOW, BLOCK), :].astype(F32)
        pooled = (sums + carry) / count
        amine[at, pl.ds(128, 128)] = ((pooled - value) * pool_gain).astype(BF16)

    def first_half(yy):
        @pl.when(yy == 0)
        def _():
            halo.arrived()
            spread(kvland[...].astype(F32), WINDOW, pl.ds(0, WINDOW))

        attend(yy, other)
        src = amine.at[rows_of((yy * 2 + other) * BLOCK, BLOCK)]
        dst = apart.at[rows_of(yy * BLOCK, BLOCK)]
        swap = one(src, dst, partner, dst)
        swap.start()
        return swap

    def product(yy, slot):
        mine = amine[rows_of((yy * 2 + c) * BLOCK, BLOCK), :]
        theirs = apart[rows_of(yy * BLOCK, BLOCK), :]
        for n in range(0, D, 512):
            cols = pl.ds(n, 512)
            got = jnp.dot(mine, wout[pl.ds(0, 256), cols], preferred_element_type=F32)
            got = got + jnp.dot(theirs, wout[pl.ds(256, 256), cols], preferred_element_type=F32)
            exact[slot, :, cols] = got
            if slot < 3:
                rounded[slot, :, cols] = got.astype(BF16)

    late = y == 2
    order = [jnp.where(late, u, v) for u, v in ((yn, yf), (yp, yn), (yf, yp))]
    at_far, at_next, at_prev = [jnp.where(late, u, v) for u, v in ((2, 0), (0, 1), (1, 2))]
    lower = [pl.ds(n * PART, PART) for n in range(HALF // PART)]
    upper = [pl.ds(HALF + n * PART, PART) for n in range(HALF // PART)]
    r_fn = [one(rounded.at[at_far, p], far_prev.at[p], up, far_prev.at[p]) for p in lower]
    r_fp = [one(rounded.at[at_far, p], far_next.at[p], down, far_next.at[p]) for p in upper]
    r_n1 = groups.new(near.at[pl.ds(HALF, HALF)])
    r_p0 = groups.new(near.at[pl.ds(0, HALF)])
    for p, q in zip(lower, upper):
        r_n1.add(rounded.at[at_next, q], near.at[q], up)
        r_p0.add(rounded.at[at_prev, p], near.at[p], down)
    r_n0 = [one(rounded.at[at_next, p], last_hbm.at[p], up, last_hbm.at[p]) for p in lower]
    r_p1 = [one(rounded.at[at_prev, p], last_hbm.at[p], down, last_hbm.at[p]) for p in upper]
    parts = range(len(lower))

    def send_far():
        for n in parts:
            r_fn[n].start()
            r_fp[n].start()

    swap_a = first_half(order[0])
    attend(order[0], c)
    swap_b = first_half(order[1])
    outs.shares.arrived()
    swap_a.arrived()
    product(order[0], 0)

    @pl.when(late)
    def _():
        r_n1.start(*parts[:EARLY])

    @pl.when(y != 2)
    def _():
        send_far()

    attend(order[1], c)
    swap_b.arrived()
    product(order[1], 1)

    @pl.when(late)
    def _():
        r_p0.start(*parts[:EARLY])

    @pl.when(y != 2)
    def _():
        r_n1.start()

    swap_c = first_half(order[2])
    attend(order[2], c)
    swap_d = first_half(y)
    swap_c.arrived()
    product(order[2], 2)

    @pl.when(late)
    def _():
        send_far()
        if EARLY < len(parts):
            r_n1.start(*parts[EARLY:])
            r_p0.start(*parts[EARLY:])

    @pl.when(y != 2)
    def _():
        r_p0.start()

    attend(y, c)
    for n in parts:
        r_fn[n].arrived()
        rounded[at_next, lower[n], :] = (
            exact[at_next, lower[n], :] + far_prev[lower[n], :].astype(F32)
        ).astype(BF16)
        r_n0[n].start()
        r_fp[n].arrived()
        rounded[at_prev, upper[n], :] = (
            exact[at_prev, upper[n], :] + far_next[upper[n], :].astype(F32)
        ).astype(BF16)
        r_p1[n].start()

    swap_d.arrived()
    product(y, 3)
    r_n1.arrived()
    r_p0.arrived()
    for p in lower + upper:
        result[p, :] = (exact[3, p, :] + near[p, :].astype(F32)).astype(BF16)
    mine = pltpu.make_async_copy(result, own_hbm, out_sems.at[0])
    mine.start()
    for n in parts:
        r_n0[n].arrived()
        r_p1[n].arrived()
    mine.wait()
    groups.all_sent(sent)

    @pl.when(y == SIDE - 1)
    def _():
        c_x.sent()
        c_z.sent()

    assert len(groups.made) == N_GROUPS, len(groups.made)


def local(
    tokens_in,
    norm_gain,
    query_weight,
    key_weight,
    value_weight,
    pool_weight,
    sink_logit,
    pool_gain,
    attention_out_weight,
    pool_out_weight,
):
    hbm = pl.BlockSpec(memory_space=pltpu.HBM)
    scratch = [
        ((BLOCK, D), BF16),
        ((1, D), F32),
        ((1, 128), F32),
        ((1, 2), F32),
        ((DEPTH, DEPTH), BF16),
        ((ROWS, D), BF16),
        ((D, IN_COLS), BF16),
        ((512, D), BF16),
        ((ROWS, 128), BF16),
        ((WINDOW, 128), BF16),
        ((WINDOW, 128), BF16),
        ((ROWS + WINDOW, 128), BF16),
        ((ROWS + WINDOW, 128), BF16),
        ((ROWS + WINDOW, 128), BF16),
        ((ROWS + WINDOW, 128), BF16),
        ((ROWS + WINDOW, 128), BF16),
        ((2 * SIDE, 8, 128), F32),
        ((1, 128), F32),
        ((1, D), F32),
        ((3, 1, D), F32),
        ((1, D), F32),
        ((1, D), F32),
        ((1, D), F32),
        ((1, D), F32),
        ((3, 1, D), F32),
        ((3, 1, D), F32),
        ((16, D), BF16),
        ((ROWS, 256), BF16),
        ((SIDE * BLOCK, 256), BF16),
        ((4, BLOCK, D), F32),
        ((3, BLOCK, D), BF16),
        ((BLOCK, D), BF16),
        ((BLOCK, D), BF16),
        ((BLOCK, D), BF16),
        ((BLOCK, D), BF16),
        ((SENT_ROWS, 128), BF16),
    ]
    own, last = pl.pallas_call(
        kernel,
        out_shape=[
            jax.ShapeDtypeStruct((BLOCK, D), BF16),
            jax.ShapeDtypeStruct((BLOCK, D), BF16),
        ],
        in_specs=[hbm] * 10,
        out_specs=[pl.BlockSpec(memory_space=pl.ANY)] * 2,
        scratch_shapes=[pltpu.VMEM(shape, kind) for shape, kind in scratch]
        + [
            pltpu.SemaphoreType.DMA((7,)),
            pltpu.SemaphoreType.DMA((1,)),
            pltpu.SemaphoreType.DMA((SEND_SEMS + 2,)),
            pltpu.SemaphoreType.DMA((N_GROUPS,)),
        ],
        compiler_params=pltpu.CompilerParams(
            collective_id=0, has_side_effects=True, vmem_limit_bytes=62 * 1024 * 1024
        ),
    )(
        tokens_in,
        norm_gain.reshape(1, D),
        query_weight,
        key_weight.T,
        value_weight.T,
        pool_weight,
        sink_logit.reshape(1, 2),
        pool_gain.reshape(1, 128),
        attention_out_weight,
        pool_out_weight,
    )
    return (own.astype(F32) + last.astype(F32)).astype(BF16)


def solution(mesh):
    in_specs = (
        P(("sp", "tp"), None),
        P(),
        P("sp", "tp"),
        P("sp", "tp"),
        P("sp", "tp"),
        P("sp", "tp"),
        P("tp"),
        P("tp"),
        P("tp", "sp"),
        P("tp", "sp"),
    )
    out_specs = P(("sp", "tp"), None)
    return jax.shard_map(local, mesh=mesh, in_specs=in_specs, out_specs=out_specs, check_vma=False)
```

```python
import math

import jax
import jax.numpy as jnp
from jax import lax
from jax.experimental import pallas as pl
from jax.experimental.pallas import tpu as pltpu
from jax.sharding import PartitionSpec as P

MESH = pl.DeviceIdType.MESH
F32 = jnp.float32
BF16 = jnp.bfloat16

D = 2048
HEAD_DIM = 64
WINDOW = 128
EPS = 1e-06
SIDE = 4
PLANE = SIDE * SIDE
BLOCK = 96
HALF = BLOCK // 2
ROWS = 2 * SIDE * BLOCK
CHUNK = 2 * BLOCK
DEPTH = D // PLANE
IN_COLS = 384
N_GROUPS = 48
SEND_SEMS = 4
SENT_ROWS = 12800
PART = 16
EARLY = 1


class Groups:
    def __init__(self, send_sems, recv_sems):
        self.send_sems, self.recv_sems, self.made, self.lone = send_sems, recv_sems, [], []

    def new(self, whole, lone=False):
        number = len(self.made)
        place = SEND_SEMS + len(self.lone) if lone else number % SEND_SEMS
        group = Group(self.send_sems.at[place], self.recv_sems.at[number], whole)
        self.made.append(group)
        if lone:
            self.lone.append(group)
        return group

    def one(self, src, dst, device, land):
        group = self.new(land)
        group.add(src, dst, device)
        return group

    def all_sent(self, rows):
        for n in range(SEND_SEMS):
            here = [g for g in self.made[n::SEND_SEMS] if g not in self.lone]
            size = sum(math.prod(g.whole.shape) * g.whole.dtype.itemsize for g in here)
            assert size % 4096 == 0 and size <= SENT_ROWS * 256, size
            part = rows.at[pl.ds(0, size // 256)]
            here[0].copy(part, part, here[0].device).wait_send()


class Group:
    def __init__(self, send_sem, recv_sem, whole):
        self.send_sem, self.recv_sem, self.whole, self.copies = send_sem, recv_sem, whole, []

    def copy(self, src, dst, device):
        return pltpu.make_async_remote_copy(
            src_ref=src,
            dst_ref=dst,
            send_sem=self.send_sem,
            recv_sem=self.recv_sem,
            device_id=device,
            device_id_type=MESH,
        )

    def add(self, src, dst, device):
        self.device = device
        self.copies.append((src, dst, device))
        return len(self.copies) - 1

    def start(self, *which):
        for n in which or range(len(self.copies)):
            self.copy(*self.copies[n]).start()

    def arrived(self):
        self.copy(self.whole, self.whole, self.device).wait_recv()

    def sent(self):
        self.copy(self.whole, self.whole, self.device).wait_send()


def rows_of(start, size, unit=16):
    return pl.ds(pl.multiple_of(start, unit), size)


def kernel(
    x_hbm,
    gain_hbm,
    wq_hbm,
    wk_hbm,
    wv_hbm,
    wp_hbm,
    sink_hbm,
    pgain_hbm,
    wa_hbm,
    wo_hbm,
    own_hbm,
    last_hbm,
    xin,
    gain,
    pgain,
    sink,
    wkv,
    tok,
    win,
    wout,
    qbuf,
    kvsend,
    kvland,
    kp0,
    kp1,
    vp0,
    vp1,
    pext,
    totals,
    before,
    cols_own,
    cols_y,
    cols_core,
    cols_other,
    cols_chip,
    cols_row,
    cols_x,
    cols_z,
    terms,
    amine,
    apart,
    exact,
    rounded,
    far_prev,
    far_next,
    near,
    result,
    sent,
    local_sems,
    out_sems,
    send_sems,
    recv_sems,
):
    sp = lax.axis_index("sp")
    tp = lax.axis_index("tp")
    z, x = sp // SIDE, lax.rem(sp, SIDE)
    y, c = tp // 2, lax.rem(tp, 2)
    other = 1 - c

    def turn(i, by):
        return lax.rem(i + by + SIDE, SIDE)

    yn, yp, yf = turn(y, 1), turn(y, -1), turn(y, 2)
    partner = (sp, y * 2 + other)
    up, down = (sp, yn * 2 + c), (sp, yp * 2 + c)

    barrier = pltpu.get_barrier_semaphore()
    beside = [(z * SIDE + turn(x, by), tp) for by in (1, -1)]
    above = [(turn(z, by) * SIDE + x, tp) for by in (1, -1)]
    opposite = [(z * SIDE + turn(x, 2), tp), (turn(z, 2) * SIDE + x, tp), (sp, yf * 2 + c)]
    peers = [up, down, partner] + beside + above + opposite
    for peer in peers:
        pl.semaphore_signal(barrier, inc=1, device_id=peer, device_id_type=MESH)

    own_in = rows_of(sp * DEPTH, DEPTH, 128)
    own_cols = rows_of(sp * 128, 128, 128)
    loads = [
        (0, x_hbm, xin),
        (1, gain_hbm, gain),
        (2, wk_hbm, wkv.at[pl.ds(0, HEAD_DIM)]),
        (2, wv_hbm, wkv.at[pl.ds(HEAD_DIM, HEAD_DIM)]),
        (3, wq_hbm, win.at[own_in, pl.ds(0, 128)]),
        (3, wp_hbm, win.at[own_in, pl.ds(256, 128)]),
        (4, wa_hbm, wout.at[pl.ds(0, 128), own_cols]),
        (4, wo_hbm, wout.at[pl.ds(128, 128), own_cols]),
        (5, pgain_hbm, pgain),
        (6, sink_hbm, sink),
    ]
    for n, src, dst in loads:
        pltpu.make_async_copy(src, dst, local_sems.at[n]).start()

    def loaded(n, whole):
        pltpu.make_async_copy(whole, whole, local_sems.at[n]).wait()

    loaded(0, xin)
    loaded(1, gain)
    gains = gain[...]

    def column_sums(rows):
        return jnp.sum(rows.astype(F32), axis=0, keepdims=True)

    columns = jnp.zeros((1, D), F32)
    for r in range(0, BLOCK, 16):
        wide = xin[pl.ds(r, 16)].astype(F32)
        inverse = lax.rsqrt(jnp.mean(wide * wide, axis=1, keepdims=True) + EPS)
        normed = (wide * inverse * gains).astype(BF16)
        tok[rows_of(tp * BLOCK + r, 16), :] = normed
        columns = columns + column_sums(normed)
    cols_own[...] = columns
    loaded(2, wkv)
    win[own_in, pl.ds(128, 128)] = wkv[...].T
    loaded(3, win.at[own_in, pl.ds(0, 256)])
    loaded(4, wout.at[pl.ds(0, 256), own_cols])
    loaded(5, pgain)
    loaded(6, sink)

    groups = Groups(send_sems, recv_sems)

    def block(yy, cc):
        return tok.at[rows_of((yy * 2 + cc) * BLOCK, BLOCK)]

    def half(yy, cc, h):
        return tok.at[rows_of((yy * 2 + cc) * BLOCK + h * HALF, HALF)]

    one = groups.one
    c_y = groups.new(cols_y)
    for n, by in enumerate((1, -1, 2)):
        c_y.add(cols_own, cols_y.at[n], (sp, turn(y, by) * 2 + c))
    t_n0 = one(half(y, c, 0), half(y, c, 0), up, half(yp, c, 0))
    t_p1 = one(half(y, c, 1), half(y, c, 1), down, half(yn, c, 1))
    t_n1 = one(half(y, c, 1), half(y, c, 1), up, half(yp, c, 1))
    t_p0 = one(half(y, c, 0), half(y, c, 0), down, half(yn, c, 0))
    f_n = one(half(yp, c, 0), half(yp, c, 0), up, half(yf, c, 0))
    f_p = one(half(yn, c, 1), half(yn, c, 1), down, half(yf, c, 1))
    d_own = one(block(y, c), block(y, c), partner, block(y, other))

    def across(yy):
        group = groups.new(block(yy, other))
        for h in range(2):
            group.add(half(yy, c, h), half(yy, c, h), partner)
        return group

    d_p, d_n, d_f = across(yp), across(yn), across(yf)
    c_core = one(cols_core, cols_other, partner, cols_other)
    c_x, c_z = groups.new(cols_x, True), groups.new(cols_z, True)
    for n, by in enumerate((1, -1, 2)):
        c_x.add(cols_chip, cols_x.at[n], (z * SIDE + turn(x, by), tp))
        c_z.add(cols_row, cols_z.at[n], (turn(z, by) * SIDE + x, tp))

    def summed(own, slots, here=None):
        total = own
        for n, by in enumerate((-1, 1, 2)):
            if here is None:
                total = total + slots[n]
            else:
                total = total + jnp.where(turn(here, by) < here, slots[n], 0.0)
        return total

    class Gather:
        def __init__(self, piece, sub, whole, direct, crossing_direct, shared=None):
            def source(g, o1, o2):
                if g == 0:
                    return turn(z, o2) * SIDE + turn(x, o1)
                return turn(z, o1) * SIDE + turn(x, o2)

            def put(group, ref, g, o1, o2):
                return group.add(ref, ref, (source(g, o1, o2), tp))

            self.first = groups.new(whole(4))
            self.first_far = groups.new(whole(2))
            self.last = groups.new(whole(8))
            self.direct = direct
            self.second, self.forward = {}, {}
            for g in range(2):
                mine = piece(g, source(g, 0, 0))
                put(self.first, mine, g, 1, 0)
                put(self.first, mine, g, -1, 0)
                if direct:
                    put(self.first_far, mine, g, 2, 0)
                else:
                    put(self.first_far, sub(g, source(g, -1, 0), 0), g, 1, 0)
                    put(self.first_far, sub(g, source(g, 1, 0), 1), g, -1, 0)
            for o in (0, -1, 1, 2):
                self.second[o] = groups.new(whole(4))
                self.forward[o] = []
                for g in range(2):
                    have = piece(g, source(g, o, 0))
                    put(self.second[o], have, g, 0, 1)
                    put(self.second[o], have, g, 0, -1)
                    if o in crossing_direct:
                        self.forward[o].append(put(self.last, have, g, 0, 2))
                    else:
                        low, high = sub(g, source(g, o, -1), 0), sub(g, source(g, o, 1), 1)
                        self.forward[o].append(put(self.last, low, g, 0, 1))
                        self.forward[o].append(put(self.last, high, g, 0, -1))
            self.crossing_direct = crossing_direct
            self.shares = None
            if shared:
                self.shares = groups.new(shared[0])
                self.share_of = {}
                for o1 in (0, -1, 1, 2):
                    for o2 in (0, -1, 1, 2):
                        self.share_of[o1, o2] = [
                            self.shares.add(
                                piece(g, source(g, o1, o2)), shared[1](g, source(g, o1, o2)), partner
                            )
                            for g in range(2)
                        ]

        def share(self, o1, o2):
            if self.shares:
                self.shares.start(*self.share_of[o1, o2])

        def begin(self):
            self.first.start()
            if self.direct:
                self.first_far.start()

        def cross(self, o):
            self.second[o].start()
            if o in self.crossing_direct:
                self.last.start(*self.forward[o])
            self.share(o, 0)

        def near(self):
            self.first.arrived()
            if not self.direct:
                self.first_far.start()
            self.cross(-1)
            self.cross(1)

        def distant(self):
            self.first_far.arrived()
            self.cross(2)

        def pass_on(self, o):
            self.second[o].arrived()
            if o not in self.crossing_direct:
                self.last.start(*self.forward[o])
            self.share(o, -1)
            self.share(o, 1)

        def finish(self):
            self.last.arrived()
            for o in (0, -1, 1, 2):
                self.share(o, 2)

    size = DEPTH // 2
    ins = Gather(
        lambda g, s: win.at[rows_of(s * DEPTH + g * size, size)],
        lambda g, s, h: win.at[rows_of(s * DEPTH + g * size + h * (size // 2), size // 2)],
        lambda n: win.at[pl.ds(0, n * size)],
        True,
        (),
    )
    outs = Gather(
        lambda g, s: wout.at[pl.ds(g * 128, 128), rows_of(s * 128, 128, 128)],
        lambda g, s, h: wout.at[pl.ds(g * 128 + h * 64, 64), rows_of(s * 128, 128, 128)],
        lambda n: wout.at[pl.ds(0, n * 8)],
        False,
        (2,),
        (
            wout.at[pl.ds(256, 256)],
            lambda g, s: wout.at[pl.ds(256 + g * 128, 128), rows_of(s * 128, 128, 128)],
        ),
    )

    pl.semaphore_wait(barrier, len(peers))

    for group in (c_y, t_n0, t_p1, t_n1, t_p0):
        group.start()
    ins.begin()
    ins.cross(0)
    outs.begin()
    outs.cross(0)
    d_own.start()
    ins.near()
    ins.distant()
    c_y.arrived()
    own_parity = summed(columns, cols_y)
    cols_core[...] = own_parity
    c_core.start()
    outs.near()
    ins.pass_on(0)
    c_core.arrived()
    cols_chip[...] = own_parity + cols_other[...]

    @pl.when(y == SIDE - 1)
    def _():
        c_x.start()

    t_n0.arrived()
    f_n.start()
    d_p.start(0)
    t_p1.arrived()
    f_p.start()
    d_n.start(1)
    outs.pass_on(0)
    ins.pass_on(-1)
    ins.pass_on(1)
    ins.pass_on(2)
    outs.distant()

    t_n1.arrived()
    d_p.start(1)
    t_p0.arrived()
    d_n.start(0)
    outs.pass_on(-1)
    outs.pass_on(1)

    @pl.when(y == SIDE - 1)
    def _():
        c_x.arrived()
        cols_row[...] = summed(cols_chip[...], cols_x)
        c_z.start()

    ins.finish()

    def spread(kv, rows, at):
        first = lax.broadcasted_iota(jnp.int32, (rows, 128), 1) < HEAD_DIM
        turned = pltpu.roll(kv, HEAD_DIM, 1)
        kp0[at, :] = jnp.where(first, kv, 0.0).astype(BF16)
        kp1[at, :] = jnp.where(first, 0.0, turned).astype(BF16)
        vp0[at, :] = jnp.where(first, turned, 0.0).astype(BF16)
        vp1[at, :] = jnp.where(first, 0.0, kv).astype(BF16)

    last = pl.ds(ROWS, WINDOW)
    after = (lax.rem(sp + 1, PLANE), tp)
    halo = groups.new(pext.at[pl.ds(0, 2 * WINDOW)])
    halo.add(kvsend, kvland, after)
    halo.add(pext.at[last], pext.at[pl.ds(0, WINDOW)], after)

    def project(yy):
        at = rows_of(yy * CHUNK, CHUNK)
        got = jnp.dot(tok[at, :], win[...], preferred_element_type=F32)
        qbuf[at, :] = got[:, :128].astype(BF16)
        ahead = rows_of(yy * CHUNK + WINDOW, CHUNK)
        spread(got[:, 128:256].astype(BF16).astype(F32), CHUNK, ahead)
        pool = got[:, 256:].astype(BF16)
        pext[ahead, :] = pool
        sums = jnp.sum(pool.astype(F32).reshape(2, BLOCK // 8, 8, 128), axis=1)
        totals[pl.ds(yy * 2, 2)] = sums

        @pl.when(yy == SIDE - 1)
        def _():
            kvsend[...] = kp0[last, :] + vp1[last, :]
            halo.start()

    f_n.arrived()
    d_f.start(0)
    f_p.arrived()
    d_f.start(1)
    d_own.arrived()
    d_p.arrived()
    d_n.arrived()
    project(jnp.where(y == 0, yp, jnp.where(y == 3, y, yn)))
    project(jnp.where(y == 3, yp, y))
    project(jnp.where((y == 0) | (y == 3), yn, yp))

    @pl.when(y == SIDE - 1)
    def _():
        c_z.arrived()
        nothing = jnp.zeros((1, D), F32)
        ahead = summed(nothing, cols_z, z) + summed(nothing, cols_x, x)
        high = ahead.astype(BF16).astype(F32)
        middle = (ahead - high).astype(BF16).astype(F32)
        low = ahead - high - middle
        term = lax.broadcasted_iota(jnp.int32, (16, D), 0)
        rest = jnp.where(term == 1, middle, jnp.where(term == 2, low, 0.0))
        terms[...] = jnp.where(term == 0, high, rest).astype(BF16)

    d_f.arrived()
    project(yf)
    outs.pass_on(2)
    outs.finish()

    @pl.when(y == SIDE - 1)
    def _():
        got = jnp.dot(terms[...], win[:, 256:], preferred_element_type=F32)
        before[...] = jnp.sum(got, axis=0, keepdims=True)

    span = WINDOW + BLOCK
    q_index = lax.broadcasted_iota(jnp.int32, (BLOCK, span), 0)
    k_index = lax.broadcasted_iota(jnp.int32, (BLOCK, span), 1)
    distance = q_index + WINDOW - k_index
    reach = jnp.where(y == 0, 8, jnp.where(y == 1, 32, jnp.where(y == 2, WINDOW, 1 << 24)))
    inside = (distance >= 0) & (distance < WINDOW)
    banded = (distance >= 0) & (distance < reach) & ((k_index >= WINDOW) | (y < 3))
    sinks = (sink[:, 0:1], sink[:, 1:2])
    pool_gain = pgain[...]

    def probabilities(q, keys, allowed, sink):
        scores = lax.dot_general(q, keys, (((1,), (1,)), ((), ())), preferred_element_type=F32)
        scores = jnp.where(allowed, scores * HEAD_DIM ** (-0.5), -jnp.inf)
        peak = jnp.maximum(jnp.max(scores, axis=1, keepdims=True), sink)
        expo = jnp.exp(scores - peak)
        denom = jnp.sum(expo, axis=1, keepdims=True) + jnp.exp(sink - peak)
        return (expo * (1.0 / denom)).astype(BF16)

    def attend(yy, cc):
        number = yy * 2 + cc
        start = sp * ROWS + number * BLOCK
        at, pair = rows_of(number * BLOCK, BLOCK), rows_of(number * BLOCK, span)
        present = k_index >= WINDOW - start
        allowed, band = inside & present, banded & present
        q = qbuf[at, :]
        p0 = probabilities(q, kp0[pair, :], allowed, sinks[0])
        p1 = probabilities(q, kp1[pair, :], allowed, sinks[1])
        mixed = jnp.dot(p0, vp0[pair, :], preferred_element_type=F32)
        mixed = mixed + jnp.dot(p1, vp1[pair, :], preferred_element_type=F32)
        amine[at, pl.ds(0, 128)] = mixed.astype(BF16)
        ones = jnp.where(band, 1.0, 0.0).astype(BF16)
        sums = jnp.dot(ones, pext[pair, :], preferred_element_type=F32)
        earlier = lax.broadcasted_iota(jnp.int32, (2 * SIDE, 8, 128), 0) < number
        carry = jnp.sum(jnp.sum(jnp.where(earlier, totals[...], 0.0), axis=0), axis=0, keepdims=True)
        carry = jnp.where(y == 3, carry + before[...], 0.0)
        position = start + lax.broadcasted_iota(jnp.int32, (BLOCK, 128), 0)
        count = jnp.minimum(position + 1, reach).astype(F32)
        value = pext[rows_of(number * BLOCK + WINDOW, BLOCK), :].astype(F32)
        pooled = (sums + carry) / count
        amine[at, pl.ds(128, 128)] = ((pooled - value) * pool_gain).astype(BF16)

    def first_half(yy):
        @pl.when(yy == 0)
        def _():
            halo.arrived()
            spread(kvland[...].astype(F32), WINDOW, pl.ds(0, WINDOW))

        attend(yy, other)
        src = amine.at[rows_of((yy * 2 + other) * BLOCK, BLOCK)]
        dst = apart.at[rows_of(yy * BLOCK, BLOCK)]
        swap = one(src, dst, partner, dst)
        swap.start()
        return swap

    def product(yy, slot):
        mine = amine[rows_of((yy * 2 + c) * BLOCK, BLOCK), :]
        theirs = apart[rows_of(yy * BLOCK, BLOCK), :]
        for n in range(0, D, 512):
            cols = pl.ds(n, 512)
            got = jnp.dot(mine, wout[pl.ds(0, 256), cols], preferred_element_type=F32)
            got = got + jnp.dot(theirs, wout[pl.ds(256, 256), cols], preferred_element_type=F32)
            exact[slot, :, cols] = got
            if slot < 3:
                rounded[slot, :, cols] = got.astype(BF16)

    late = y == 2
    order = [jnp.where(late, u, v) for u, v in ((yn, yf), (yp, yn), (yf, yp))]
    at_far, at_next, at_prev = [jnp.where(late, u, v) for u, v in ((2, 0), (0, 1), (1, 2))]
    lower = [pl.ds(n * PART, PART) for n in range(HALF // PART)]
    upper = [pl.ds(HALF + n * PART, PART) for n in range(HALF // PART)]
    r_fn = [one(rounded.at[at_far, p], far_prev.at[p], up, far_prev.at[p]) for p in lower]
    r_fp = [one(rounded.at[at_far, p], far_next.at[p], down, far_next.at[p]) for p in upper]
    r_n1 = groups.new(near.at[pl.ds(HALF, HALF)])
    r_p0 = groups.new(near.at[pl.ds(0, HALF)])
    for p, q in zip(lower, upper):
        r_n1.add(rounded.at[at_next, q], near.at[q], up)
        r_p0.add(rounded.at[at_prev, p], near.at[p], down)
    r_n0 = [one(rounded.at[at_next, p], last_hbm.at[p], up, last_hbm.at[p]) for p in lower]
    r_p1 = [one(rounded.at[at_prev, p], last_hbm.at[p], down, last_hbm.at[p]) for p in upper]
    parts = range(len(lower))

    def send_far():
        for n in parts:
            r_fn[n].start()
            r_fp[n].start()

    swap_a = first_half(order[0])
    attend(order[0], c)
    swap_b = first_half(order[1])
    outs.shares.arrived()
    swap_a.arrived()
    product(order[0], 0)

    @pl.when(late)
    def _():
        r_n1.start(*parts[:EARLY])

    @pl.when(y != 2)
    def _():
        send_far()

    attend(order[1], c)
    swap_b.arrived()
    product(order[1], 1)

    @pl.when(late)
    def _():
        r_p0.start(*parts[:EARLY])

    @pl.when(y != 2)
    def _():
        r_n1.start()

    swap_c = first_half(order[2])
    attend(order[2], c)
    swap_d = first_half(y)
    swap_c.arrived()
    product(order[2], 2)

    @pl.when(late)
    def _():
        send_far()
        if EARLY < len(parts):
            r_n1.start(*parts[EARLY:])
            r_p0.start(*parts[EARLY:])

    @pl.when(y != 2)
    def _():
        r_p0.start()

    attend(y, c)
    for n in parts:
        r_fn[n].arrived()
        rounded[at_next, lower[n], :] = (
            exact[at_next, lower[n], :] + far_prev[lower[n], :].astype(F32)
        ).astype(BF16)
        r_n0[n].start()
        r_fp[n].arrived()
        rounded[at_prev, upper[n], :] = (
            exact[at_prev, upper[n], :] + far_next[upper[n], :].astype(F32)
        ).astype(BF16)
        r_p1[n].start()

    swap_d.arrived()
    product(y, 3)
    r_n1.arrived()
    r_p0.arrived()
    for p in lower + upper:
        result[p, :] = (exact[3, p, :] + near[p, :].astype(F32)).astype(BF16)
    mine = pltpu.make_async_copy(result, own_hbm, out_sems.at[0])
    mine.start()
    for n in parts:
        r_n0[n].arrived()
        r_p1[n].arrived()
    mine.wait()
    groups.all_sent(sent)

    @pl.when(y == SIDE - 1)
    def _():
        c_x.sent()
        c_z.sent()

    assert len(groups.made) == N_GROUPS, len(groups.made)


def local(
    tokens_in,
    norm_gain,
    query_weight,
    key_weight,
    value_weight,
    pool_weight,
    sink_logit,
    pool_gain,
    attention_out_weight,
    pool_out_weight,
):
    hbm = pl.BlockSpec(memory_space=pltpu.HBM)
    scratch = [
        ((BLOCK, D), BF16),
        ((1, D), F32),
        ((1, 128), F32),
        ((1, 2), F32),
        ((DEPTH, DEPTH), BF16),
        ((ROWS, D), BF16),
        ((D, IN_COLS), BF16),
        ((512, D), BF16),
        ((ROWS, 128), BF16),
        ((WINDOW, 128), BF16),
        ((WINDOW, 128), BF16),
        ((ROWS + WINDOW, 128), BF16),
        ((ROWS + WINDOW, 128), BF16),
        ((ROWS + WINDOW, 128), BF16),
        ((ROWS + WINDOW, 128), BF16),
        ((ROWS + WINDOW, 128), BF16),
        ((2 * SIDE, 8, 128), F32),
        ((1, 128), F32),
        ((1, D), F32),
        ((3, 1, D), F32),
        ((1, D), F32),
        ((1, D), F32),
        ((1, D), F32),
        ((1, D), F32),
        ((3, 1, D), F32),
        ((3, 1, D), F32),
        ((16, D), BF16),
        ((ROWS, 256), BF16),
        ((SIDE * BLOCK, 256), BF16),
        ((4, BLOCK, D), F32),
        ((3, BLOCK, D), BF16),
        ((BLOCK, D), BF16),
        ((BLOCK, D), BF16),
        ((BLOCK, D), BF16),
        ((BLOCK, D), BF16),
        ((SENT_ROWS, 128), BF16),
    ]
    own, last = pl.pallas_call(
        kernel,
        out_shape=[
            jax.ShapeDtypeStruct((BLOCK, D), BF16),
            jax.ShapeDtypeStruct((BLOCK, D), BF16),
        ],
        in_specs=[hbm] * 10,
        out_specs=[pl.BlockSpec(memory_space=pl.ANY)] * 2,
        scratch_shapes=[pltpu.VMEM(shape, kind) for shape, kind in scratch]
        + [
            pltpu.SemaphoreType.DMA((7,)),
            pltpu.SemaphoreType.DMA((1,)),
            pltpu.SemaphoreType.DMA((SEND_SEMS + 2,)),
            pltpu.SemaphoreType.DMA((N_GROUPS,)),
        ],
        compiler_params=pltpu.CompilerParams(
            collective_id=0, has_side_effects=True, vmem_limit_bytes=62 * 1024 * 1024
        ),
    )(
        tokens_in,
        norm_gain.reshape(1, D),
        query_weight,
        key_weight.T,
        value_weight.T,
        pool_weight,
        sink_logit.reshape(1, 2),
        pool_gain.reshape(1, 128),
        attention_out_weight,
        pool_out_weight,
    )
    return (own.astype(F32) + last.astype(F32)).astype(BF16)


def solution(mesh):
    in_specs = (
        P(("sp", "tp"), None),
        P(),
        P("sp", "tp"),
        P("sp", "tp"),
        P("sp", "tp"),
        P("sp", "tp"),
        P("tp"),
        P("tp"),
        P("tp", "sp"),
        P("tp", "sp"),
    )
    out_specs = P(("sp", "tp"), None)
    return jax.shard_map(local, mesh=mesh, in_specs=in_specs, out_specs=out_specs, check_vma=False)
```
